32 devices in a mesh: ra: 4 (over z), cb: 4 (over y, x), dp: 2 (over core).
Axes of the slice: x: 2, y: 2, z: 4, core: 2. Of those that a mesh axis runs over, the one named last changes fastest.
Arguments:
- carried: bfloat16 [3072, 4096], P('dp', 'ra'), may hold values from -100 to 100
- branch_in: bfloat16 [3072, 4096], P('dp', 'ra'), may hold values from -12 to 12
- gain_in: float32 [4096], P('ra'), may hold values from 0.1 to 1.9
- bias_in: float32 [4096], P('ra'), may hold values from -1.8 to 1.8
- up_weight: bfloat16 [4096, 16384], P('ra', 'cb'), may hold values from -0.125 to 0.125
- down_weight: bfloat16 [16384, 4096], P('cb', 'ra'), may hold values from -0.046875 to 0.046875
- gain_out: float32 [4096], P('ra'), may hold values from 0.1 to 1.9
- bias_out: float32 [4096], P('ra'), may hold values from -1.8 to 1.8
Outputs:
- layer_out: bfloat16 [3072, 4096], P('dp', 'ra')
The draws below stay inside these ranges and needn't reach their ends.
All inputs are finite; a program needn't handle non-finite values.
Results may differ from the reference program's by a relative error of at most 0.006.
Values may be sent and summed in bfloat16 or wider, within the bound.
A program may use at most 128 MiB of HBM per device.

```python
import math
import jax
import jax.numpy as jnp
from jax import lax

D = 4096
FF = 16384
TOKENS = 3072


def draw_carried(key, part):
    keys = jax.random.split(jax.random.fold_in(key, 11), 3)
    columns = jnp.arange(D, dtype=jnp.float32) / D
    column_scale = 0.5 * 3.0 ** columns * jnp.exp(jax.random.uniform(keys[1], (D,), jnp.float32, -0.5, 0.5))
    values = jnp.clip(jax.random.normal(keys[0], (TOKENS, D), jnp.float32), -4.0, 4.0)
    row_scale = jnp.exp(jax.random.uniform(keys[2], (TOKENS, 1), jnp.float32, 0.0, math.log(10.0)))
    return (values * row_scale * column_scale[None, :]).astype(jnp.bfloat16)


def raised(entries, key, source, target, blocks, factor):
    owner, partner = [(jnp.arange(entries.shape[axis_at]) // (entries.shape[axis_at] // blocks)).reshape([-1 if axis == axis_at else 1 for axis in range(entries.ndim)]) for axis_at in (source, target)]
    chosen = jax.random.permutation(key, blocks)[partner]
    strong = (owner == chosen) | (owner == (partner + blocks // 2) % blocks)
    return jnp.where(strong, factor * entries, entries)


def level_of(stream_key, extent, cuts, least, high):
    level = 1.0
    for position, parts in cuts:
        steps = jax.random.uniform(jax.random.fold_in(jax.random.fold_in(stream_key, 6), position), (parts,), jnp.float32, least / len(cuts), high / len(cuts))
        level = level * jnp.repeat(jnp.exp(steps), extent[position] // parts).reshape((-1,) + (1,) * (len(extent) - 1 - position))
    return level


def noise(stream_key, shape, deviation, limit, cuts=(), held_as=jnp.bfloat16):
    drawn = deviation * jax.random.normal(stream_key, shape, jnp.float32)
    if cuts:
        drawn = drawn * level_of(stream_key, shape, cuts, -0.22, 0.18)
    return jnp.clip(drawn, -limit, limit).astype(held_as)


def heavy_noise(rng, extent, scale, reach, shards, heavy, held_as=jnp.bfloat16):
    array = scale * jax.random.normal(rng, extent, jnp.float32)
    if shards:
        array = array * level_of(rng, extent, shards, -0.22, 0.18)
    return jnp.clip(raised(array, jax.random.fold_in(rng, 3), *heavy), -reach, reach).astype(held_as)


def setup_inputs(seed: int = 0) -> dict:
    seeds = jax.random.split(jax.random.key(seed), 9)
    return {
        "carried": draw_carried(jax.random.fold_in(seeds[8], 71), 0),
        "branch_in": noise(seeds[1], (TOKENS, D), 2.0, 12.0, ((0, 2), (1, 4))),
        "gain_in": jnp.clip(1.0 + 0.18 * jax.random.normal(seeds[2], (D,), jnp.float32), 0.1, 1.9),
        "bias_in": noise(seeds[3], (D,), 0.3, 1.8, ((0, 4),), jnp.float32),
        "up_weight": heavy_noise(seeds[4], (D, FF), D ** -0.5, 0.125, ((0, 4), (1, 4)), (0, 1, 4, 2.0)),
        "down_weight": noise(seeds[5], (FF, D), FF ** -0.5, 0.046875, ((0, 4), (1, 4))),
        "gain_out": jnp.clip(1.0 + 0.18 * jax.random.normal(seeds[6], (D,), jnp.float32), 0.1, 1.9),
        "bias_out": noise(seeds[7], (D,), 0.3, 1.8, ((0, 4),), jnp.float32),
    }


residual_scale = 2.0 ** 0.25
norm_eps = 1e-05

def layer_norm(mixed, gain, bias):
    mean = lax.optimization_barrier(jnp.mean(mixed, axis=-1, keepdims=True))
    spread = lax.optimization_barrier(jnp.mean(mixed * mixed, axis=-1, keepdims=True)) - mean * mean
    return (mixed - mean) * jax.lax.rsqrt(spread + norm_eps) * gain + bias

def reference(carried, branch_in, gain_in, bias_in, up_weight, down_weight, gain_out, bias_out):
    mixed_in = residual_scale * carried.astype(jnp.float32) + branch_in.astype(jnp.float32)
    normed = layer_norm(mixed_in, gain_in, bias_in).astype(jnp.bfloat16)
    pre = jnp.dot(normed, up_weight, preferred_element_type=jnp.float32)
    hidden = jnp.square(jnp.maximum(pre, 0.0)).astype(jnp.bfloat16)
    branch_out = jnp.dot(hidden, down_weight, preferred_element_type=jnp.float32)
    mixed_out = residual_scale * normed.astype(jnp.float32) + branch_out
    return layer_norm(mixed_out, gain_out, bias_out).astype(jnp.bfloat16)
```

```python
import functools
import math

import jax
import jax.numpy as jnp
from jax import lax
from jax.experimental import pallas as pl
from jax.experimental.pallas import tpu as pltpu
from jax.sharding import PartitionSpec as P

residual_scale = 2.0**0.25
norm_eps = 1e-05
tile_cap = 256
lag_x, lag_a, lag_z = 2, 4, 6
lead = 2


def kernel(n, m, tile, carried_hbm, branch_hbm, w1_hbm, w2_hbm, gain_in_ref, bias_in_ref, gain_ref,
           bias_ref, o_hbm, s1_src, s1_recv, s1_tot, xh, xres, w1s, w2s, h, psend, yrecv, zsend,
           zrecv, fin, acc, st_src, st_recv, loc_sem, s1_sem, w1_sem, w2_sem, xz_sem, xy_sem,
           y_sem, z_sem, ag_sem, st_send, st_rcv, out_sem):
    me, cb, dp = lax.axis_index("ra"), lax.axis_index("cb"), lax.axis_index("dp")
    tokens, dl = xres.shape
    fs = h.shape[2]
    q = tokens // m
    chunks = tokens // 128
    qchunks = q // 128
    rounds1, rounds2 = fs // tile, dl // tile
    tiles = rounds2 * n
    width = n * dl
    xb, yb = lax.rem(cb, 2), cb // 2
    px, py = cb + 1 - 2 * xb, lax.rem(cb + 2, m)
    sib = 1 - dp

    def slot_of(c):
        return lax.rem(c, 2) * 2 + c // 2

    def at_rows(start, size):
        return pl.ds(pl.multiple_of(start, size), size)

    def remote(src, dst, send, recv, to):
        return pltpu.make_async_remote_copy(
            src_ref=src, dst_ref=dst, send_sem=send, recv_sem=recv, device_id=to)

    barrier = pltpu.get_barrier_semaphore()
    for o in range(n):
        for c in range(m):
            if o or c:
                pl.semaphore_signal(barrier, inc=1, device_id={
                    "ra": lax.rem(me + o, n), "cb": lax.rem(cb + c, m)})
    pl.semaphore_signal(barrier, inc=1, device_id={"dp": sib})

    own_carried = pltpu.make_async_copy(carried_hbm, fin, loc_sem.at[0])
    own_branch = pltpu.make_async_copy(branch_hbm, psend.at[pl.ds(0, tokens)], loc_sem.at[1])
    own_w1 = pltpu.make_async_copy(w1_hbm.at[:, at_rows(me * fs, fs)], w1s.at[0, me], loc_sem.at[2])
    own_w2 = pltpu.make_async_copy(w2_hbm.at[at_rows(me * fs, fs)], w2s.at[0, me], loc_sem.at[3])
    own_carried.start()
    own_branch.start()
    own_w1.start()
    own_w2.start()
    pl.semaphore_wait(barrier, n * m)

    class Stream:
        def __init__(self, buf, sem, block):
            self.buf, self.sem, self.block = buf, sem, block
            half = buf.shape[2] // 2
            self.rows = at_rows(dp * half, half)
            self.other = at_rows(sib * half, half)

        def ref(self, share, src, p, rows):
            return self.buf.at[share, src, rows, at_rows(p * tile, tile)]

        def z(self, to, p):
            return remote(self.block(to, p), self.ref(0, me, p, self.rows),
                          self.sem.at[0, to, p], self.sem.at[1, me, p], {"ra": to})

        def z_landed(self, src, p):
            ref = self.ref(0, src, p, self.rows)
            return remote(ref, ref, self.sem.at[0, src, p], self.sem.at[1, src, p], {"ra": src})

        def x(self, src, p):
            ref = self.ref(0, src, p, self.rows)
            return remote(ref, self.ref(1, src, p, self.rows), self.sem.at[2, src, p],
                          self.sem.at[3, src, p], {"cb": px})

        def x_own(self, p):
            return remote(self.block(me, p), self.ref(1, me, p, self.rows), self.sem.at[2, me, p],
                          self.sem.at[3, me, p], {"cb": px})

        def pair(self, share, src, p):
            ref = self.ref(share, src, p, self.rows)
            return remote(ref, ref, self.sem.at[4 + 2 * share, src, p],
                          self.sem.at[5 + 2 * share, src, p], {"dp": sib})

        def pair_landed(self, share, src, p):
            ref = self.ref(share, src, p, self.other)
            return remote(ref, ref, self.sem.at[4 + 2 * share, src, p],
                          self.sem.at[5 + 2 * share, src, p], {"dp": sib})

        def send(self, p, least=1, most=n - 1):
            for o in range(least, most + 1):
                @pl.when(me + o < n)
                def _():
                    self.z(me + o, p).start()

                @pl.when(me >= o)
                def _():
                    self.z(me - o, p).start()

        def forward(self, src, p):
            @pl.when(src != me)
            def _():
                self.z_landed(src, p).wait_recv()
                self.x(src, p).start()
                self.pair(0, src, p).start()

        def forward_near(self, p):
            for o in range(1, n):
                @pl.when(me + o < n)
                def _():
                    self.forward(me + o, p)

                @pl.when(me >= o)
                def _():
                    self.forward(me - o, p)

        def share(self, src, p):
            self.x(src, p).wait_recv()
            self.pair(1, src, p).start()

        def ready(self, src, p):
            @pl.when(src != me)
            def _():
                self.pair_landed(0, src, p).wait_recv()
            self.pair_landed(1, src, p).wait_recv()

        def sent(self, src, p):
            @pl.when(src != me)
            def _():
                self.z(src, p).wait_send()
                self.pair(0, src, p).wait_send()
            self.x(src, p).wait_send()
            self.pair(1, src, p).wait_send()

    one = Stream(w1s, w1_sem, lambda to, p: w1_hbm.at[
        at_rows(dp * (dl // 2), dl // 2), at_rows(to * fs + p * tile, tile)])
    two = Stream(w2s, w2_sem, lambda to, p: w2_hbm.at[
        at_rows(to * fs + dp * (fs // 2), fs // 2), at_rows(p * tile, tile)])

    one.send(0, 1, 1)
    for p in range(rounds1):
        one.x_own(p).start()

    def s1_copy(o):
        return remote(s1_src, s1_recv.at[me], s1_sem.at[0, o], s1_sem.at[1, me],
                      {"ra": lax.rem(me + o, n)})

    def s1_landed(o):
        sender = lax.rem(me + o, n)
        ref = s1_recv.at[sender]
        return remote(ref, ref, s1_sem.at[0, o], s1_sem.at[1, sender], {"ra": sender})

    def mixed_in(here):
        return residual_scale * fin[here, :].astype(jnp.float32) + psend[here, :].astype(
            jnp.float32)

    def sums_of(total):
        lane = lax.broadcasted_iota(jnp.int32, (128, 128), 1)
        return jnp.where(
            lane < 64, jnp.sum(total, axis=1, keepdims=True),
            jnp.sum(total * total, axis=1, keepdims=True)).T

    def column(row):
        return jnp.broadcast_to(row, (128, 128)).T[:, 0:1]

    st_src[...] = jnp.zeros_like(st_src)
    own_carried.wait()
    own_branch.wait()

    @pl.loop(0, chunks)
    def _(c):
        sums = sums_of(mixed_in(at_rows(c * 128, 128)))
        s1_src[pl.ds(c, 1), :] = sums[0:1, :]
        s1_src[pl.ds(chunks + c, 1), :] = sums[64:65, :]
    for o in range(1, n):
        s1_copy(o).start()
    if n > 2:
        one.send(0, 2, 2)
    s1_tot[...] = s1_src[...]
    for o in range(1, n):
        s1_landed(o).wait_recv()
        s1_tot[...] += s1_recv[lax.rem(me + o, n)]

    def normed(c):
        mean_row = s1_tot[pl.ds(c, 1), :] / width
        scale_row = lax.rsqrt(s1_tot[pl.ds(chunks + c, 1), :] / width - mean_row * mean_row + norm_eps)
        here = at_rows(c * 128, 128)
        out = ((mixed_in(here) - column(mean_row)) * column(scale_row) * gain_in_ref[...]
               + bias_in_ref[...]).astype(jnp.bfloat16)
        xres[here, :] = out
        return out

    def normed_half(first, count):
        @pl.loop(0, count)
        def _(c):
            local = first + c
            xh[me, at_rows(local * 128, 128), :] = normed(xb * 2 * qchunks + local)

    normed_half(yb * qchunks, qchunks)

    def xz(src, to_right):
        ref = xh.at[src, at_rows(yb * q, q)]
        return remote(ref, ref, xz_sem.at[0 if to_right else 1, src], xz_sem.at[2, src], {
            "ra": jnp.minimum(me + 1, n - 1) if to_right else jnp.maximum(me - 1, 0)})

    def xy(src):
        ref = xh.at[src, at_rows(yb * q, q)]
        return remote(ref, ref, xy_sem.at[0, src], xy_sem.at[1, src], {"cb": py})

    def xy_landed(src):
        ref = xh.at[src, at_rows((1 - yb) * q, q)]
        return remote(ref, ref, xy_sem.at[0, src], xy_sem.at[1, src], {"cb": py})

    def from_left(s):
        @pl.when(me >= s)
        def _():
            xz(me - s, True).wait_recv()

            @pl.when(me + 1 < n)
            def _():
                xz(me - s, True).start()
            xy(me - s).start()

    def from_right(s):
        @pl.when(me + s < n)
        def _():
            xz(me + s, False).wait_recv()

            @pl.when(me >= 1)
            def _():
                xz(me + s, False).start()
            xy(me + s).start()

    @pl.when(me + 1 < n)
    def _():
        xz(me, True).start()

    @pl.when(me >= 1)
    def _():
        xz(me, False).start()
    if n > 3:
        one.send(0, 3)
    if rounds1 > 1:
        one.send(1)
    normed_half((1 - yb) * qchunks, qchunks)

    @pl.loop(0, 2 * qchunks)
    def _(c):
        normed((1 - xb) * 2 * qchunks + c)

    one.forward_near(0)
    two.x_own(0).start()
    for s in range(1, max(n, rounds1)):
        if s < n:
            from_left(s)
            from_right(s)
        if s + 1 < rounds1:
            one.send(s + 1)
        if s < rounds2:
            two.x_own(s).start()
        if s < rounds1 - 1:
            one.forward_near(s)
            for src in range(n):
                one.share(src, s - 1)
    for p in range(n, rounds2):
        two.x_own(p).start()
    for p in range(min(lead, rounds2)):
        two.send(p)

    own_w1.wait()
    for src in range(n):
        @pl.when(src != me)
        def _():
            xy_landed(src).wait_recv()

    def up(p):
        for src in range(n):
            one.ready(src, p)
        cols = at_rows(p * tile, tile)
        for share in range(2):
            @pl.loop(0, 2)
            def _(b):
                here = at_rows(b * q, q)
                total = jnp.dot(xh[0, here, :], w1s[share, 0, :, cols],
                                preferred_element_type=jnp.float32)
                for k in range(1, n):
                    total += jnp.dot(xh[k, here, :], w1s[share, k, :, cols],
                                     preferred_element_type=jnp.float32)
                h[share, here, cols] = jnp.square(jnp.maximum(total, 0.0)).astype(jnp.bfloat16)

    @pl.loop(0, max(rounds1 - 2, 0))
    def _(p):
        up(p)
    if rounds1 > 1:
        one.forward_near(rounds1 - 1)
        for src in range(n):
            one.share(src, rounds1 - 2)
        up(rounds1 - 2)
    for src in range(n):
        one.share(src, rounds1 - 1)
    up(rounds1 - 1)
    own_w2.wait()

    def where_of(t):
        return t // n, lax.rem(t, n)

    def out_tile(ref, block, r):
        return ref.at[at_rows(block * q, q), at_rows(r * tile, tile)]

    def down(start, d, r):
        cols = at_rows(r * tile, tile)
        here = at_rows(start, q)
        return (jnp.dot(h[0, here, :], w2s[0, d, :, cols], preferred_element_type=jnp.float32)
                + jnp.dot(h[1, here, :], w2s[1, d, :, cols], preferred_element_type=jnp.float32))

    def y_copy(t):
        r, d = where_of(t)
        return remote(out_tile(psend, d, r), out_tile(yrecv, d, r), y_sem.at[0, t], y_sem.at[1, t],
                      {"cb": py})

    def z_copy(t, to_right):
        r, d = where_of(t)
        to = jnp.minimum(me + 1, n - 1) if to_right else jnp.maximum(me - 1, 0)
        block = d if to_right else jnp.where(d == to, n, d)
        return remote(out_tile(zsend, d, r), out_tile(zrecv, block, r), z_sem.at[0, t],
                      z_sem.at[1 if to_right else 2, t], {"ra": to})

    def z_landed(t, to_right):
        r, d = where_of(t)
        block = d if to_right else jnp.where(d == me, n, d)
        ref = out_tile(zrecv, block, r)
        return remote(ref, ref, z_sem.at[0, t], z_sem.at[1 if to_right else 2, t], {
            "ra": jnp.maximum(me - 1, 0) if to_right else jnp.minimum(me + 1, n - 1)})

    def ag_copy(r, o):
        ref = out_tile(fin, slot_of(cb), r)
        return remote(ref, ref, ag_sem.at[0, r, o], ag_sem.at[1, r, cb], {"cb": lax.rem(cb + o, m)})

    def ag_landed(r, o):
        sender = lax.rem(cb + o, m)
        ref = out_tile(fin, slot_of(sender), r)
        return remote(ref, ref, ag_sem.at[0, r, o], ag_sem.at[1, r, sender], {"cb": sender})

    def st_copy(o, c):
        return remote(st_src, st_recv.at[me, cb], st_send.at[o, c], st_rcv.at[me, cb],
                      {"ra": lax.rem(me + o, n), "cb": lax.rem(cb + c, m)})

    def st_landed(o, c):
        z, s = lax.rem(me + o, n), lax.rem(cb + c, m)
        ref = st_recv.at[z, s]
        return remote(ref, ref, st_send.at[o, c], st_rcv.at[z, s], {"ra": z, "cb": s})

    def stage_r(t):
        r, d = where_of(t)
        two.forward(d, r)

    def stage_x(t):
        r, d = where_of(t)
        two.share(d, r)

    def stage_a(t):
        r, d = where_of(t)
        two.ready(d, r)
        out_tile(psend, d, r)[...] = down((1 - yb) * q, d, r).astype(jnp.bfloat16)
        y_copy(t).start()

    def stage_z(t):
        r, d = where_of(t)
        acc[...] = down(yb * q, d, r)
        y_copy(t).wait_recv()
        acc[...] += out_tile(yrecv, d, r)[...].astype(jnp.float32)

        @pl.when((me >= 1) & (d >= me))
        def _():
            z_landed(t, True).wait_recv()
            acc[...] += out_tile(zrecv, d, r)[...].astype(jnp.float32)

        @pl.when((me + 1 < n) & (d <= me))
        def _():
            z_landed(t, False).wait_recv()
            acc[...] += out_tile(zrecv, jnp.where(d == me, n, d), r)[...].astype(jnp.float32)

        @pl.when(d != me)
        def _():
            out_tile(zsend, d, r)[...] = acc[...].astype(jnp.bfloat16)

        @pl.when(d > me)
        def _():
            z_copy(t, True).start()

        @pl.when(d < me)
        def _():
            z_copy(t, False).start()

        @pl.when(d == me)
        def _():
            out_tile(fin, slot_of(cb), r)[...] = acc[...].astype(jnp.bfloat16)
            for o in range(1, m):
                ag_copy(r, o).start()
            for c in range(qchunks):
                sums = sums_of(acc[pl.ds(c * 128, 128), :] + residual_scale * xres[
                    at_rows(slot_of(cb) * q + c * 128, 128), at_rows(r * tile, tile)].astype(
                        jnp.float32))
                st_src[pl.ds(c, 1), :] += sums[0:1, :]
                st_src[pl.ds(qchunks + c, 1), :] += sums[64:65, :]

            @pl.when(r == rounds2 - 1)
            def _():
                for o in range(n):
                    for c in range(m):
                        if o or c:
                            st_copy(o, c).start()

    @pl.loop(0, tiles + lag_z + n - 1)
    def _(step):
        for r in range(lead, rounds2):
            @pl.when(step == (r - lead + 1) * n)
            def _():
                two.send(r)
        for lag, stage in ((0, stage_r), (lag_x, stage_x), (lag_a, stage_a)):
            @pl.when((step >= lag) & (step < tiles + lag))
            def _():
                stage(step - lag)

        @pl.loop(0, n)
        def _(back):
            hop = n - 1 - back
            t = step - lag_z - hop
            d = lax.rem(t + n * n, n)
            mine = jnp.where(d > me, me, jnp.where(
                d < me, n - 1 - me, jnp.maximum(me, n - 1 - me)))

            @pl.when((t >= 0) & (t < tiles) & (mine == hop))
            def _():
                stage_z(t)

    for o in range(n):
        for c in range(m):
            if o or c:
                st_landed(o, c).wait_recv()
    st_recv[me, cb] = st_src[...]
    for o in range(1, m):
        for r in range(rounds2):
            ag_landed(r, o).wait_recv()

    def out_copy(c):
        here = at_rows(c * 128, 128)
        return pltpu.make_async_copy(xres.at[here], o_hbm.at[here], out_sem.at[c])

    for slot in range(m):
        owner = slot // 2 + 2 * (slot % 2)
        total = st_recv[0, owner]
        for z in range(1, n):
            total += st_recv[z, owner]
        s1_tot[pl.ds(0, 2 * qchunks), :] = total[0:2 * qchunks, :]

        @pl.loop(0, qchunks)
        def _(c):
            mean_row = s1_tot[pl.ds(c, 1), :] / width
            scale_row = lax.rsqrt(
                s1_tot[pl.ds(qchunks + c, 1), :] / width - mean_row * mean_row + norm_eps)
            here = at_rows(slot * q + c * 128, 128)
            mixed = residual_scale * xres[here, :].astype(jnp.float32) + fin[here, :].astype(
                jnp.float32)
            xres[here, :] = ((mixed - column(mean_row)) * column(scale_row) * gain_ref[...]
                             + bias_ref[...]).astype(jnp.bfloat16)
            out_copy(slot * qchunks + c).start()

    for src in range(n):
        @pl.when((src == me) | (src < me))
        def _():
            @pl.when(me + 1 < n)
            def _():
                xz(src, True).wait_send()

        @pl.when((src == me) | (src > me))
        def _():
            @pl.when(me >= 1)
            def _():
                xz(src, False).wait_send()

        @pl.when(src != me)
        def _():
            xy(src).wait_send()

        for stream, count in ((one, rounds1), (two, rounds2)):
            @pl.loop(0, count)
            def _(p):
                stream.sent(src, p)
    for o in range(1, n):
        s1_copy(o).wait_send()

    @pl.loop(0, tiles)
    def _(t):
        d = lax.rem(t, n)
        y_copy(t).wait_send()

        @pl.when(d != me)
        def _():
            z_copy(t, True).wait_send()

    for o in range(1, m):
        for r in range(rounds2):
            ag_copy(r, o).wait_send()
    for o in range(n):
        for c in range(m):
            if o or c:
                st_copy(o, c).wait_send()

    @pl.loop(0, chunks)
    def _(c):
        out_copy(c).wait()


def per_device(carried, branch_in, gain_in, bias_in, up_weight, down_weight, gain_out, bias_out):
    n, m, nd = lax.axis_size("ra"), lax.axis_size("cb"), lax.axis_size("dp")
    tokens, dl = carried.shape
    fs = up_weight.shape[1] // n
    assert m == 4 and nd == 2 and tokens % (128 * m) == 0 and tokens // m <= 512
    q = tokens // m
    tile = math.gcd(tile_cap, math.gcd(fs, dl))
    rounds1, rounds2 = fs // tile, dl // tile
    tiles = rounds2 * n
    chunk_rows = -(-2 * (tokens // 128) // 8) * 8
    dma = pltpu.SemaphoreType.DMA
    bf16, f32 = jnp.bfloat16, jnp.float32
    hbm = pl.BlockSpec(memory_space=pl.ANY)
    vmem = pl.BlockSpec(memory_space=pltpu.VMEM)
    return pl.pallas_call(
        functools.partial(kernel, n, m, tile),
        out_shape=jax.ShapeDtypeStruct((tokens, dl), bf16),
        in_specs=[hbm, hbm, hbm, hbm, vmem, vmem, vmem, vmem],
        out_specs=hbm,
        scratch_shapes=[
            pltpu.VMEM((chunk_rows, 128), f32),
            pltpu.VMEM((n, chunk_rows, 128), f32),
            pltpu.VMEM((chunk_rows, 128), f32),
            pltpu.VMEM((n, 2 * q, dl), bf16),
            pltpu.VMEM((tokens, dl), bf16),
            pltpu.VMEM((2, n, dl, fs), bf16),
            pltpu.VMEM((2, n, fs, dl), bf16),
            pltpu.VMEM((2, 2 * q, fs), bf16),
            pltpu.VMEM((max(n, m) * q, dl), bf16),
            pltpu.VMEM((n * q, dl), bf16),
            pltpu.VMEM((n * q, dl), bf16),
            pltpu.VMEM(((n + 1) * q, dl), bf16),
            pltpu.VMEM((tokens, dl), bf16),
            pltpu.VMEM((q, tile), f32),
            pltpu.VMEM((8, 128), f32),
            pltpu.VMEM((n, m, 8, 128), f32),
            dma((4,)), dma((2, n)), dma((8, n, rounds1)), dma((8, n, rounds2)), dma((3, n)),
            dma((2, n)), dma((2, tiles)), dma((3, tiles)), dma((2, rounds2, m)), dma((n, m)),
            dma((n, m)), dma((tokens // 128,)),
        ],
        compiler_params=pltpu.CompilerParams(
            collective_id=0, has_side_effects=True, vmem_limit_bytes=67 * 1000 * 1000),
    )(carried, branch_in, up_weight, down_weight, gain_in.reshape(1, dl), bias_in.reshape(1, dl),
      gain_out.reshape(1, dl), bias_out.reshape(1, dl))


def solution(mesh):
    in_specs = (
        P("dp", "ra"),
        P("dp", "ra"),
        P("ra"),
        P("ra"),
        P("ra", "cb"),
        P("cb", "ra"),
        P("ra"),
        P("ra"),
    )
    out_specs = P("dp", "ra")
    return jax.shard_map(
        per_device, mesh=mesh, in_specs=in_specs, out_specs=out_specs, check_vma=False
    )
```

```python
import functools
import math

import jax
import jax.numpy as jnp
from jax import lax
from jax.experimental import pallas as pl
from jax.experimental.pallas import tpu as pltpu
from jax.sharding import PartitionSpec as P

residual_scale = 2.0**0.25
norm_eps = 1e-05
tile_cap = 256
tile2_cap = 128
lag_x, lag_a, lag_z, lag_hop, lag_late = 3, 8, 14, 4, 12
lead = 3
lead_mid = 5
near = 3
early = 2
lag_g = 1


def kernel(n, m, tile, tile2, carried_hbm, branch_hbm, w1_hbm, w2_hbm, gain_in_ref, bias_in_ref, gain_ref,
           bias_ref, o_hbm, s1_src, s1_recv, s1_tot, xh, xres, w1s, w2s, h, psend, yrecv, zsend,
           zrecv, fin, acc, st_src, st_recv, loc_sem, s1_sem, w1_sem, w2_sem, xz_sem, xy_sem,
           y_sem, z_sem, ag_sem, st_send, st_rcv, out_sem, meet_sem):
    me, cb, dp = lax.axis_index("ra"), lax.axis_index("cb"), lax.axis_index("dp")
    tokens, dl = xres.shape
    fs = h.shape[2]
    q = tokens // m
    chunks = tokens // 128
    qchunks = q // 128
    rounds1, rounds2 = fs // tile, dl // tile2
    tiles = rounds2 * n
    first = min(early, rounds1)
    width = n * dl
    xb, yb = lax.rem(cb, 2), cb // 2
    px, py = cb + 1 - 2 * xb, lax.rem(cb + 2, m)
    sib = 1 - dp

    def slot_of(c):
        return lax.rem(c, 2) * 2 + c // 2

    def at_rows(start, size):
        return pl.ds(pl.multiple_of(start, size), size)

    def remote(src, dst, send, recv, to):
        return pltpu.make_async_remote_copy(
            src_ref=src, dst_ref=dst, send_sem=send, recv_sem=recv, device_id=to)

    barrier = pltpu.get_barrier_semaphore()
    for o in range(n):
        for c in range(m):
            if o or c:
                pl.semaphore_signal(barrier, inc=1, device_id={
                    "ra": lax.rem(me + o, n), "cb": lax.rem(cb + c, m)})
    pl.semaphore_signal(barrier, inc=1, device_id={"dp": sib})

    own_carried = pltpu.make_async_copy(carried_hbm, fin, loc_sem.at[0])
    own_branch = pltpu.make_async_copy(branch_hbm, psend.at[pl.ds(0, tokens)], loc_sem.at[1])
    own_w1 = pltpu.make_async_copy(w1_hbm.at[:, at_rows(me * fs, fs)], w1s.at[0, me], loc_sem.at[2])
    own_w2 = pltpu.make_async_copy(w2_hbm.at[at_rows(me * fs, fs)], w2s.at[0, me], loc_sem.at[3])
    own_carried.start()
    own_branch.start()
    own_w1.start()
    own_w2.start()
    pl.semaphore_wait(barrier, n * m)

    class Stream:
        def __init__(self, buf, sem, tile, block):
            self.buf, self.sem, self.tile, self.block = buf, sem, tile, block
            half = buf.shape[2] // 2
            self.rows = at_rows(dp * half, half)
            self.other = at_rows(sib * half, half)

        def ref(self, share, src, p, rows):
            return self.buf.at[share, src, rows, at_rows(p * self.tile, self.tile)]

        def z(self, to, p):
            return remote(self.block(to, p), self.ref(0, me, p, self.rows),
                          self.sem.at[0, to, p], self.sem.at[1, me, p], {"ra": to})

        def z_landed(self, src, p):
            ref = self.ref(0, src, p, self.rows)
            return remote(ref, ref, self.sem.at[0, src, p], self.sem.at[1, src, p], {"ra": src})

        def x(self, src, p):
            ref = self.ref(0, src, p, self.rows)
            return remote(ref, self.ref(1, src, p, self.rows), self.sem.at[2, src, p],
                          self.sem.at[3, src, p], {"cb": px})

        def x_own(self, p):
            return remote(self.block(me, p), self.ref(1, me, p, self.rows), self.sem.at[2, me, p],
                          self.sem.at[3, me, p], {"cb": px})

        def pair(self, share, src, p):
            ref = self.ref(share, src, p, self.rows)
            return remote(ref, ref, self.sem.at[4 + 2 * share, src, p],
                          self.sem.at[5 + 2 * share, src, p], {"dp": sib})

        def pair_landed(self, share, src, p):
            ref = self.ref(share, src, p, self.other)
            return remote(ref, ref, self.sem.at[4 + 2 * share, src, p],
                          self.sem.at[5 + 2 * share, src, p], {"dp": sib})

        def right(self, p, least, most):
            for o in range(least, most + 1):
                @pl.when(me + o < n)
                def _():
                    self.z(me + o, p).start()

        def left(self, p, least, most):
            for o in range(least, most + 1):
                @pl.when(me >= o)
                def _():
                    self.z(me - o, p).start()

        def send(self, p, least=1, most=n - 1):
            for o in range(least, most + 1):
                self.right(p, o, o)
                self.left(p, o, o)

        def forward(self, src, p):
            self.z_landed(src, p).wait_recv()
            self.x(src, p).start()
            self.pair(0, src, p).start()

        def forward_from(self, o, p):
            @pl.when(me + o < n)
            def _():
                self.forward(me + o, p)

            @pl.when(me >= o)
            def _():
                self.forward(me - o, p)

        def share_from(self, o, p):
            @pl.when(me + o < n)
            def _():
                self.share(me + o, p)

            @pl.when(me >= o)
            def _():
                self.share(me - o, p)

        def share(self, src, p):
            self.x(src, p).wait_recv()
            self.pair(1, src, p).start()

        def ready(self, src, p):
            @pl.when(src != me)
            def _():
                self.pair_landed(0, src, p).wait_recv()
            self.pair_landed(1, src, p).wait_recv()

        def sent(self, src, p):
            @pl.when(src != me)
            def _():
                self.z(src, p).wait_send()
                self.pair(0, src, p).wait_send()
            self.x(src, p).wait_send()
            self.pair(1, src, p).wait_send()

    one = Stream(w1s, w1_sem, tile, lambda to, p: w1_hbm.at[
        at_rows(dp * (dl // 2), dl // 2), at_rows(to * fs + p * tile, tile)])
    two = Stream(w2s, w2_sem, tile2, lambda to, p: w2_hbm.at[
        at_rows(to * fs + dp * (fs // 2), fs // 2), at_rows(p * tile2, tile2)])

    one.send(0, 1, 1)
    for p in range(rounds1):
        one.x_own(p).start()

    def s1_copy(o):
        return remote(s1_src, s1_recv.at[me], s1_sem.at[0, o], s1_sem.at[1, me],
                      {"ra": lax.rem(me + o, n)})

    def s1_landed(o):
        sender = lax.rem(me + o, n)
        ref = s1_recv.at[sender]
        return remote(ref, ref, s1_sem.at[0, o], s1_sem.at[1, sender], {"ra": sender})

    def mixed_in(here):
        return residual_scale * fin[here, :].astype(jnp.float32) + psend[here, :].astype(
            jnp.float32)

    def sums_of(total):
        lane = lax.broadcasted_iota(jnp.int32, (128, 128), 1)
        return jnp.where(
            lane < 64, jnp.sum(total, axis=1, keepdims=True),
            jnp.sum(total * total, axis=1, keepdims=True)).T

    def column(row):
        return jnp.broadcast_to(row, (128, 128)).T[:, 0:1]

    st_src[...] = jnp.zeros_like(st_src)
    own_carried.wait()
    own_branch.wait()

    @pl.loop(0, chunks)
    def _(c):
        sums = sums_of(mixed_in(at_rows(c * 128, 128)))
        s1_src[pl.ds(c, 1), :] = sums[0:1, :]
        s1_src[pl.ds(chunks + c, 1), :] = sums[64:65, :]
    for o in range(1, n):
        s1_copy(o).start()
    for p in range(1, first):
        one.send(p, 1, 1)
    s1_tot[...] = s1_src[...]
    for o in range(1, n):
        s1_landed(o).wait_recv()
        s1_tot[...] += s1_recv[lax.rem(me + o, n)]

    def normed(c):
        mean_row = s1_tot[pl.ds(c, 1), :] / width
        scale_row = lax.rsqrt(s1_tot[pl.ds(chunks + c, 1), :] / width - mean_row * mean_row + norm_eps)
        here = at_rows(c * 128, 128)
        out = ((mixed_in(here) - column(mean_row)) * column(scale_row) * gain_in_ref[...]
               + bias_in_ref[...]).astype(jnp.bfloat16)
        xres[here, :] = out
        return out

    def normed_half(first, count):
        @pl.loop(0, count)
        def _(c):
            local = first + c
            xh[me, at_rows(local * 128, 128), :] = normed(xb * 2 * qchunks + local)

    normed_half(yb * qchunks, qchunks)

    def xz(src, to_right):
        ref = xh.at[src, at_rows(yb * q, q)]
        return remote(ref, ref, xz_sem.at[0 if to_right else 1, src], xz_sem.at[2, src], {
            "ra": jnp.minimum(me + 1, n - 1) if to_right else jnp.maximum(me - 1, 0)})

    def xy(src):
        ref = xh.at[src, at_rows(yb * q, q)]
        return remote(ref, ref, xy_sem.at[0, src], xy_sem.at[1, src], {"cb": py})

    def xy_landed(src):
        ref = xh.at[src, at_rows((1 - yb) * q, q)]
        return remote(ref, ref, xy_sem.at[0, src], xy_sem.at[1, src], {"cb": py})

    def from_left(s):
        @pl.when(me >= s)
        def _():
            xz(me - s, True).wait_recv()

            @pl.when(me + 1 < n)
            def _():
                xz(me - s, True).start()
            xy(me - s).start()

    def from_right(s):
        @pl.when(me + s < n)
        def _():
            xz(me + s, False).wait_recv()

            @pl.when(me >= 1)
            def _():
                xz(me + s, False).start()
            xy(me + s).start()

    def meet():
        pl.semaphore_signal(meet_sem, inc=1, device_id={"dp": sib})
        pl.semaphore_wait(meet_sem, 1)

    def after_relays(s):
        @pl.when(me == s)
        def _():
            for p in range(first, rounds1):
                one.right(p, 1, 1)

        @pl.when(me == n - 1 - s)
        def _():
            for p in range(first, rounds1):
                one.left(p, 1, 1)
        for o in range(2, n):
            @pl.when(me + o == s)
            def _():
                for p in range(rounds1):
                    one.right(p, o, o)

            @pl.when(me - o == n - 1 - s)
            def _():
                for p in range(rounds1):
                    one.left(p, o, o)

    @pl.when(me + 1 < n)
    def _():
        xz(me, True).start()

    @pl.when(me >= 1)
    def _():
        xz(me, False).start()
    after_relays(0)
    normed_half((1 - yb) * qchunks, qchunks)

    @pl.loop(0, 2 * qchunks)
    def _(c):
        normed((1 - xb) * 2 * qchunks + c)

    for p in range(first):
        one.forward_from(1, p)
    for p in range(rounds2):
        two.x_own(p).start()
    for s in range(1, n):
        from_left(s)
        from_right(s)
        meet()
        after_relays(s)
    for p in range(min(near, rounds2)):
        two.send(p, 1, 1)
    for p in range(rounds1):
        one.share(me, p)
    for p in range(first):
        one.share_from(1, p)

    own_w1.wait()

    def up(p):
        for src in range(n):
            one.ready(src, p)
        cols = at_rows(p * tile, tile)
        for share in range(2):
            @pl.loop(0, 2)
            def _(b):
                here = at_rows(b * q, q)
                total = jnp.dot(xh[0, here, :], w1s[share, 0, :, cols],
                                preferred_element_type=jnp.float32)
                for k in range(1, n):
                    total += jnp.dot(xh[k, here, :], w1s[share, k, :, cols],
                                     preferred_element_type=jnp.float32)
                h[share, here, cols] = jnp.square(jnp.maximum(total, 0.0)).astype(jnp.bfloat16)

    def far(step, ends, p):
        for o in range(2, n):
            for src in (me - o, me + o):
                end = (src == 0) | (src == n - 1)

                @pl.when((src >= 0) & (src < n) & (end if ends else jnp.logical_not(end)))
                def _():
                    step(src, p)

    def close(step, ends, p):
        for src in (me - 1, me + 1):
            end = (src == 0) | (src == n - 1) | (me == 0) | (me == n - 1)

            @pl.when((src >= 0) & (src < n) & (end if ends else jnp.logical_not(end)))
            def _():
                step(src, p)

    groups = [(close, True, p) for p in range(first, rounds1)]
    groups += [(far, True, p) for p in range(rounds1)]
    groups += [(close, False, p) for p in range(first, rounds1)]
    groups += [(far, False, p) for p in range(rounds1)]
    done = 0

    def share_group(i):
        which, ends, p = groups[i]
        which(one.share, ends, p)

    for i, (which, ends, p) in enumerate(groups):
        which(one.forward, ends, p)
        if i == min(rounds1, len(groups) - 1):
            for src in range(n):
                @pl.when(src != me)
                def _():
                    xy_landed(src).wait_recv()
        if i >= lag_g:
            share_group(i - lag_g)
            after = i - lag_g - (len(groups) - rounds1)
            if after >= 0 and i + 1 < len(groups):
                up(after)
                done = after + 1
    ahead = jnp.where((me == 0) | (me == n - 1), min(lead, rounds2), min(lead_mid, rounds2))

    def send_two(r):
        @pl.when(r >= near)
        def _():
            two.send(r, 1, 1)
        two.send(r, 2, n - 1)

    @pl.loop(0, ahead)
    def _(r):
        send_two(r)
    for i in range(max(len(groups) - lag_g, 0), len(groups)):
        share_group(i)
        after = i - (len(groups) - rounds1)
        while done <= after:
            up(done)
            done += 1
    own_w2.wait()

    def where_of(t):
        at = lax.rem(t + 4 * n * n, n)
        return t // n, jnp.where(lax.rem(at, 2) == 0, at // 2, n - 1 - at // 2)

    def out_tile(ref, block, r):
        return ref.at[at_rows(block * q, q), at_rows(r * tile2, tile2)]

    def down(start, d, r):
        cols = at_rows(r * tile2, tile2)
        here = at_rows(start, q)
        return (jnp.dot(h[0, here, :], w2s[0, d, :, cols], preferred_element_type=jnp.float32)
                + jnp.dot(h[1, here, :], w2s[1, d, :, cols], preferred_element_type=jnp.float32))

    def y_copy(t):
        r, d = where_of(t)
        return remote(out_tile(psend, d, r), out_tile(yrecv, d, r), y_sem.at[0, t], y_sem.at[1, t],
                      {"cb": py})

    def z_copy(t, to_right):
        r, d = where_of(t)
        to = jnp.minimum(me + 1, n - 1) if to_right else jnp.maximum(me - 1, 0)
        block = d if to_right else jnp.where(d == to, n, d)
        return remote(out_tile(zsend, d, r), out_tile(zrecv, block, r), z_sem.at[0, t],
                      z_sem.at[1 if to_right else 2, t], {"ra": to})

    def z_landed(t, to_right):
        r, d = where_of(t)
        block = d if to_right else jnp.where(d == me, n, d)
        ref = out_tile(zrecv, block, r)
        return remote(ref, ref, z_sem.at[0, t], z_sem.at[1 if to_right else 2, t], {
            "ra": jnp.maximum(me - 1, 0) if to_right else jnp.minimum(me + 1, n - 1)})

    def ag_copy(r, o):
        ref = out_tile(fin, slot_of(cb), r)
        return remote(ref, ref, ag_sem.at[0, r, o], ag_sem.at[1, r, cb], {"cb": lax.rem(cb + o, m)})

    def ag_landed(r, o):
        sender = lax.rem(cb + o, m)
        ref = out_tile(fin, slot_of(sender), r)
        return remote(ref, ref, ag_sem.at[0, r, o], ag_sem.at[1, r, sender], {"cb": sender})

    def st_copy(o, c):
        return remote(st_src, st_recv.at[me, cb], st_send.at[o, c], st_rcv.at[me, cb],
                      {"ra": lax.rem(me + o, n), "cb": lax.rem(cb + c, m)})

    def st_landed(o, c):
        z, s = lax.rem(me + o, n), lax.rem(cb + c, m)
        ref = st_recv.at[z, s]
        return remote(ref, ref, st_send.at[o, c], st_rcv.at[z, s], {"ra": z, "cb": s})

    def source_of(t):
        at = lax.rem(t, n)
        return jnp.where(at < 2, at, n + 1 - at)

    def stage_r(t):
        o = source_of(t)

        @pl.when(o > 0)
        def _():
            two.forward_from(o, t // n)

    def stage_x(t):
        o = source_of(t)

        @pl.when(o > 0)
        def _():
            two.share_from(o, t // n)

        @pl.when(o == 0)
        def _():
            two.share(me, t // n)

    def stage_a(t):
        r, d = where_of(t)
        two.ready(d, r)
        out_tile(psend, d, r)[...] = down((1 - yb) * q, d, r).astype(jnp.bfloat16)
        y_copy(t).start()

    def stage_z(t):
        r, d = where_of(t)
        acc[...] = down(yb * q, d, r)
        y_copy(t).wait_recv()
        acc[...] += out_tile(yrecv, d, r)[...].astype(jnp.float32)

        @pl.when((me >= 1) & (d >= me))
        def _():
            z_landed(t, True).wait_recv()
            acc[...] += out_tile(zrecv, d, r)[...].astype(jnp.float32)

        @pl.when((me + 1 < n) & (d <= me))
        def _():
            z_landed(t, False).wait_recv()
            acc[...] += out_tile(zrecv, jnp.where(d == me, n, d), r)[...].astype(jnp.float32)

        @pl.when(d != me)
        def _():
            out_tile(zsend, d, r)[...] = acc[...].astype(jnp.bfloat16)

        @pl.when(d > me)
        def _():
            z_copy(t, True).start()

        @pl.when(d < me)
        def _():
            z_copy(t, False).start()

        @pl.when(d == me)
        def _():
            out_tile(fin, slot_of(cb), r)[...] = acc[...].astype(jnp.bfloat16)
            for c in range(qchunks):
                sums = sums_of(acc[pl.ds(c * 128, 128), :] + residual_scale * xres[
                    at_rows(slot_of(cb) * q + c * 128, 128), at_rows(r * tile2, tile2)].astype(
                        jnp.float32))
                st_src[pl.ds(c, 1), :] += sums[0:1, :]
                st_src[pl.ds(qchunks + c, 1), :] += sums[64:65, :]

            @pl.when(r == rounds2 - 1)
            def _():
                for o in range(n):
                    for c in range(m):
                        if o or c:
                            st_copy(o, c).start()
            for o in range(1, m):
                ag_copy(r, o).start()

    def lag_of(hop):
        return lag_z + hop * lag_hop + jnp.where(2 * hop >= n, lag_late, 0)

    @pl.loop(0, tiles + lag_z + (n - 1) * lag_hop + lag_late)
    def _(step):
        for lag, stage in ((0, stage_r), (lag_x, stage_x), (lag_a, stage_a)):
            @pl.when((step >= lag) & (step < tiles + lag))
            def _():
                stage(step - lag)
            if stage is stage_r:
                late = (step + 1) // n - 1 + ahead

                @pl.when((lax.rem(step + 1, n) == 0) & (late < rounds2))
                def _():
                    send_two(late)

        @pl.loop(0, n)
        def _(back):
            hop = n - 1 - back
            t = step - lag_of(hop)
            d = where_of(t)[1]
            mine = jnp.where(d > me, me, jnp.where(
                d < me, n - 1 - me, jnp.maximum(me, n - 1 - me)))

            @pl.when((t >= 0) & (t < tiles) & (mine == hop))
            def _():
                stage_z(t)

    for o in range(n):
        for c in range(m):
            if o or c:
                st_landed(o, c).wait_recv()
    st_recv[me, cb] = st_src[...]
    for o in range(1, m):
        for r in range(rounds2):
            ag_landed(r, o).wait_recv()

    def out_copy(c):
        here = at_rows(c * 128, 128)
        return pltpu.make_async_copy(xres.at[here], o_hbm.at[here], out_sem.at[c])

    for slot in range(m):
        owner = slot // 2 + 2 * (slot % 2)
        total = st_recv[0, owner]
        for z in range(1, n):
            total += st_recv[z, owner]
        s1_tot[pl.ds(0, 2 * qchunks), :] = total[0:2 * qchunks, :]

        @pl.loop(0, qchunks)
        def _(c):
            mean_row = s1_tot[pl.ds(c, 1), :] / width
            scale_row = lax.rsqrt(
                s1_tot[pl.ds(qchunks + c, 1), :] / width - mean_row * mean_row + norm_eps)
            here = at_rows(slot * q + c * 128, 128)
            mixed = residual_scale * xres[here, :].astype(jnp.float32) + fin[here, :].astype(
                jnp.float32)
            xres[here, :] = ((mixed - column(mean_row)) * column(scale_row) * gain_ref[...]
                             + bias_ref[...]).astype(jnp.bfloat16)
            out_copy(slot * qchunks + c).start()

    for src in range(n):
        @pl.when((src == me) | (src < me))
        def _():
            @pl.when(me + 1 < n)
            def _():
                xz(src, True).wait_send()

        @pl.when((src == me) | (src > me))
        def _():
            @pl.when(me >= 1)
            def _():
                xz(src, False).wait_send()

        @pl.when(src != me)
        def _():
            xy(src).wait_send()

        for stream, count in ((one, rounds1), (two, rounds2)):
            @pl.loop(0, count)
            def _(p):
                stream.sent(src, p)
    for o in range(1, n):
        s1_copy(o).wait_send()

    @pl.loop(0, tiles)
    def _(t):
        d = where_of(t)[1]
        y_copy(t).wait_send()

        @pl.when(d != me)
        def _():
            z_copy(t, True).wait_send()

    for o in range(1, m):
        for r in range(rounds2):
            ag_copy(r, o).wait_send()
    for o in range(n):
        for c in range(m):
            if o or c:
                st_copy(o, c).wait_send()

    @pl.loop(0, chunks)
    def _(c):
        out_copy(c).wait()


def per_device(carried, branch_in, gain_in, bias_in, up_weight, down_weight, gain_out, bias_out):
    n, m, nd = lax.axis_size("ra"), lax.axis_size("cb"), lax.axis_size("dp")
    tokens, dl = carried.shape
    fs = up_weight.shape[1] // n
    assert m == 4 and nd == 2 and tokens % (128 * m) == 0 and tokens // m <= 512
    q = tokens // m
    tile = math.gcd(tile_cap, math.gcd(fs, dl))
    tile2 = math.gcd(tile2_cap, dl)
    rounds1, rounds2 = fs // tile, dl // tile2
    tiles = rounds2 * n
    chunk_rows = -(-2 * (tokens // 128) // 8) * 8
    dma = pltpu.SemaphoreType.DMA
    bf16, f32 = jnp.bfloat16, jnp.float32
    hbm = pl.BlockSpec(memory_space=pl.ANY)
    vmem = pl.BlockSpec(memory_space=pltpu.VMEM)
    return pl.pallas_call(
        functools.partial(kernel, n, m, tile, tile2),
        out_shape=jax.ShapeDtypeStruct((tokens, dl), bf16),
        in_specs=[hbm, hbm, hbm, hbm, vmem, vmem, vmem, vmem],
        out_specs=hbm,
        scratch_shapes=[
            pltpu.VMEM((chunk_rows, 128), f32),
            pltpu.VMEM((n, chunk_rows, 128), f32),
            pltpu.VMEM((chunk_rows, 128), f32),
            pltpu.VMEM((n, 2 * q, dl), bf16),
            pltpu.VMEM((tokens, dl), bf16),
            pltpu.VMEM((2, n, dl, fs), bf16),
            pltpu.VMEM((2, n, fs, dl), bf16),
            pltpu.VMEM((2, 2 * q, fs), bf16),
            pltpu.VMEM((max(n, m) * q, dl), bf16),
            pltpu.VMEM((n * q, dl), bf16),
            pltpu.VMEM((n * q, dl), bf16),
            pltpu.VMEM(((n + 1) * q, dl), bf16),
            pltpu.VMEM((tokens, dl), bf16),
            pltpu.VMEM((q, tile2), f32),
            pltpu.VMEM((8, 128), f32),
            pltpu.VMEM((n, m, 8, 128), f32),
            dma((4,)), dma((2, n)), dma((8, n, rounds1)), dma((8, n, rounds2)), dma((3, n)),
            dma((2, n)), dma((2, tiles)), dma((3, tiles)), dma((2, rounds2, m)), dma((n, m)),
            dma((n, m)), dma((tokens // 128,)), pltpu.SemaphoreType.REGULAR,
        ],
        compiler_params=pltpu.CompilerParams(
            collective_id=0, has_side_effects=True, vmem_limit_bytes=67 * 1000 * 1000),
    )(carried, branch_in, up_weight, down_weight, gain_in.reshape(1, dl), bias_in.reshape(1, dl),
      gain_out.reshape(1, dl), bias_out.reshape(1, dl))


def solution(mesh):
    in_specs = (
        P("dp", "ra"),
        P("dp", "ra"),
        P("ra"),
        P("ra"),
        P("ra", "cb"),
        P("cb", "ra"),
        P("ra"),
        P("ra"),
    )
    out_specs = P("dp", "ra")
    return jax.shard_map(
        per_device, mesh=mesh, in_specs=in_specs, out_specs=out_specs, check_vma=False
    )
```

```python
import functools
import math

import jax
import jax.numpy as jnp
from jax import lax
from jax.experimental import pallas as pl
from jax.experimental.pallas import tpu as pltpu
from jax.sharding import PartitionSpec as P

residual_scale = 2.0**0.25
norm_eps = 1e-05
tile_cap = 256
tile2_cap = 128
lag_x, lag_a, lag_z, lag_hop, lag_late = 3, 7, 14, 8, 0
lead = 3
lead_mid = 5
near = 3
early = 2
lag_g = 1


def kernel(n, m, tile, tile2, carried_hbm, branch_hbm, w1_hbm, w2_hbm, gain_in_ref, bias_in_ref, gain_ref,
           bias_ref, o_hbm, s1_src, s1_recv, s1_tot, xh, xres, w1s, w2s, h, psend, yrecv, zsend,
           zrecv, fin, both, acc, st_src, st_recv, loc_sem, s1_sem, w1_sem, w2_sem, xz_sem, xy_sem,
           y_sem, z_sem, ag_sem, st_send, st_rcv, out_sem, meet_sem):
    me, cb, dp = lax.axis_index("ra"), lax.axis_index("cb"), lax.axis_index("dp")
    tokens, dl = xres.shape
    fs = h.shape[2]
    q = tokens // m
    chunks = tokens // 128
    qchunks = q // 128
    rounds1, rounds2 = fs // tile, dl // tile2
    tiles = rounds2 * n
    first = min(early, rounds1)
    width = n * dl
    xb, yb = lax.rem(cb, 2), cb // 2
    px, py = cb + 1 - 2 * xb, lax.rem(cb + 2, m)
    sib = 1 - dp

    def slot_of(c):
        return lax.rem(c, 2) * 2 + c // 2

    def at_rows(start, size):
        return pl.ds(pl.multiple_of(start, size), size)

    def remote(src, dst, send, recv, to):
        return pltpu.make_async_remote_copy(
            src_ref=src, dst_ref=dst, send_sem=send, recv_sem=recv, device_id=to)

    barrier = pltpu.get_barrier_semaphore()
    for o in range(n):
        for c in range(m):
            if o or c:
                pl.semaphore_signal(barrier, inc=1, device_id={
                    "ra": lax.rem(me + o, n), "cb": lax.rem(cb + c, m)})
    pl.semaphore_signal(barrier, inc=1, device_id={"dp": sib})

    own_carried = pltpu.make_async_copy(carried_hbm, fin, loc_sem.at[0])
    own_branch = pltpu.make_async_copy(branch_hbm, psend.at[pl.ds(0, tokens)], loc_sem.at[1])
    own_w1 = pltpu.make_async_copy(w1_hbm.at[:, at_rows(me * fs, fs)], w1s.at[0, me], loc_sem.at[2])
    own_w2 = pltpu.make_async_copy(w2_hbm.at[at_rows(me * fs, fs)], w2s.at[0, me], loc_sem.at[3])
    own_carried.start()
    own_branch.start()
    own_w1.start()
    own_w2.start()
    pl.semaphore_wait(barrier, n * m)

    class Stream:
        def __init__(self, buf, sem, tile, block):
            self.buf, self.sem, self.tile, self.block = buf, sem, tile, block
            half = buf.shape[2] // 2
            self.rows = at_rows(dp * half, half)
            self.other = at_rows(sib * half, half)

        def ref(self, share, src, p, rows):
            return self.buf.at[share, src, rows, at_rows(p * self.tile, self.tile)]

        def z(self, to, p):
            return remote(self.block(to, p), self.ref(0, me, p, self.rows),
                          self.sem.at[0, to, p], self.sem.at[1, me, p], {"ra": to})

        def z_landed(self, src, p):
            ref = self.ref(0, src, p, self.rows)
            return remote(ref, ref, self.sem.at[0, src, p], self.sem.at[1, src, p], {"ra": src})

        def x(self, src, p):
            ref = self.ref(0, src, p, self.rows)
            return remote(ref, self.ref(1, src, p, self.rows), self.sem.at[2, src, p],
                          self.sem.at[3, src, p], {"cb": px})

        def x_own(self, p):
            return remote(self.block(me, p), self.ref(1, me, p, self.rows), self.sem.at[2, me, p],
                          self.sem.at[3, me, p], {"cb": px})

        def pair(self, share, src, p):
            ref = self.ref(share, src, p, self.rows)
            return remote(ref, ref, self.sem.at[4 + 2 * share, src, p],
                          self.sem.at[5 + 2 * share, src, p], {"dp": sib})

        def pair_landed(self, share, src, p):
            ref = self.ref(share, src, p, self.other)
            return remote(ref, ref, self.sem.at[4 + 2 * share, src, p],
                          self.sem.at[5 + 2 * share, src, p], {"dp": sib})

        def right(self, p, least, most):
            for o in range(least, most + 1):
                @pl.when(me + o < n)
                def _():
                    self.z(me + o, p).start()

        def left(self, p, least, most):
            for o in range(least, most + 1):
                @pl.when(me >= o)
                def _():
                    self.z(me - o, p).start()

        def send(self, p, least=1, most=n - 1):
            for o in range(least, most + 1):
                self.right(p, o, o)
                self.left(p, o, o)

        def forward(self, src, p):
            self.z_landed(src, p).wait_recv()
            self.x(src, p).start()
            self.pair(0, src, p).start()

        def forward_from(self, o, p):
            @pl.when(me + o < n)
            def _():
                self.forward(me + o, p)

            @pl.when(me >= o)
            def _():
                self.forward(me - o, p)

        def share_from(self, o, p):
            @pl.when(me + o < n)
            def _():
                self.share(me + o, p)

            @pl.when(me >= o)
            def _():
                self.share(me - o, p)

        def share(self, src, p):
            self.x(src, p).wait_recv()
            self.pair(1, src, p).start()

        def ready(self, src, p):
            @pl.when(src != me)
            def _():
                self.pair_landed(0, src, p).wait_recv()
            self.pair_landed(1, src, p).wait_recv()

        def sent(self, src, p):
            @pl.when(src != me)
            def _():
                self.z(src, p).wait_send()
                self.pair(0, src, p).wait_send()
            self.x(src, p).wait_send()
            self.pair(1, src, p).wait_send()

    one = Stream(w1s, w1_sem, tile, lambda to, p: w1_hbm.at[
        at_rows(dp * (dl // 2), dl // 2), at_rows(to * fs + p * tile, tile)])
    two = Stream(w2s, w2_sem, tile2, lambda to, p: w2_hbm.at[
        at_rows(to * fs + dp * (fs // 2), fs // 2), at_rows(p * tile2, tile2)])

    one.send(0, 1, 1)
    for p in range(rounds1):
        one.x_own(p).start()

    def s1_copy(o):
        return remote(s1_src, s1_recv.at[me], s1_sem.at[0, o], s1_sem.at[1, me],
                      {"ra": lax.rem(me + o, n)})

    def s1_landed(o):
        sender = lax.rem(me + o, n)
        ref = s1_recv.at[sender]
        return remote(ref, ref, s1_sem.at[0, o], s1_sem.at[1, sender], {"ra": sender})

    def mixed_in(here):
        return residual_scale * fin[here, :].astype(jnp.float32) + psend[here, :].astype(
            jnp.float32)

    def sums_of(total):
        lane = lax.broadcasted_iota(jnp.int32, (128, 128), 1)
        return jnp.where(
            lane < 64, jnp.sum(total, axis=1, keepdims=True),
            jnp.sum(total * total, axis=1, keepdims=True)).T

    def column(row):
        return jnp.broadcast_to(row, (128, 128)).T[:, 0:1]

    st_src[...] = jnp.zeros_like(st_src)
    own_carried.wait()
    own_branch.wait()

    @pl.loop(0, chunks)
    def _(c):
        sums = sums_of(mixed_in(at_rows(c * 128, 128)))
        s1_src[pl.ds(c, 1), :] = sums[0:1, :]
        s1_src[pl.ds(chunks + c, 1), :] = sums[64:65, :]
    for o in range(1, n):
        s1_copy(o).start()
    for p in range(1, first):
        one.send(p, 1, 1)
    s1_tot[...] = s1_src[...]
    for o in range(1, n):
        s1_landed(o).wait_recv()
        s1_tot[...] += s1_recv[lax.rem(me + o, n)]

    def normed(c):
        mean_row = s1_tot[pl.ds(c, 1), :] / width
        scale_row = lax.rsqrt(s1_tot[pl.ds(chunks + c, 1), :] / width - mean_row * mean_row + norm_eps)
        here = at_rows(c * 128, 128)
        out = ((mixed_in(here) - column(mean_row)) * column(scale_row) * gain_in_ref[...]
               + bias_in_ref[...]).astype(jnp.bfloat16)
        xres[here, :] = out
        return out

    def normed_half(first, count):
        @pl.loop(0, count)
        def _(c):
            local = first + c
            xh[me, at_rows(local * 128, 128), :] = normed(xb * 2 * qchunks + local)

    normed_half(yb * qchunks, qchunks)

    def xz(src, to_right):
        ref = xh.at[src, at_rows(yb * q, q)]
        return remote(ref, ref, xz_sem.at[0 if to_right else 1, src], xz_sem.at[2, src], {
            "ra": jnp.minimum(me + 1, n - 1) if to_right else jnp.maximum(me - 1, 0)})

    def xy(src):
        ref = xh.at[src, at_rows(yb * q, q)]
        return remote(ref, ref, xy_sem.at[0, src], xy_sem.at[1, src], {"cb": py})

    def xy_landed(src):
        ref = xh.at[src, at_rows((1 - yb) * q, q)]
        return remote(ref, ref, xy_sem.at[0, src], xy_sem.at[1, src], {"cb": py})

    def from_left(s):
        @pl.when(me >= s)
        def _():
            xz(me - s, True).wait_recv()

            @pl.when(me + 1 < n)
            def _():
                xz(me - s, True).start()
            xy(me - s).start()

    def from_right(s):
        @pl.when(me + s < n)
        def _():
            xz(me + s, False).wait_recv()

            @pl.when(me >= 1)
            def _():
                xz(me + s, False).start()
            xy(me + s).start()

    def meet():
        pl.semaphore_signal(meet_sem, inc=1, device_id={"dp": sib})
        pl.semaphore_wait(meet_sem, 1)

    def after_relays(s):
        @pl.when(me == s)
        def _():
            for p in range(first, rounds1):
                one.right(p, 1, 1)

        @pl.when(me == n - 1 - s)
        def _():
            for p in range(first, rounds1):
                one.left(p, 1, 1)
        for o in range(2, n):
            @pl.when(me + o == s)
            def _():
                for p in range(rounds1):
                    one.right(p, o, o)

            @pl.when(me - o == n - 1 - s)
            def _():
                for p in range(rounds1):
                    one.left(p, o, o)

    @pl.when(me + 1 < n)
    def _():
        xz(me, True).start()

    @pl.when(me >= 1)
    def _():
        xz(me, False).start()
    after_relays(0)
    normed_half((1 - yb) * qchunks, qchunks)

    @pl.loop(0, 2 * qchunks)
    def _(c):
        normed((1 - xb) * 2 * qchunks + c)

    for p in range(first):
        one.forward_from(1, p)
    for p in range(rounds2):
        two.x_own(p).start()
    for s in range(1, n):
        from_left(s)
        from_right(s)
        meet()
        after_relays(s)
    for p in range(min(near, rounds2)):
        two.send(p, 1, 1)
    for p in range(rounds1):
        one.share(me, p)
    for p in range(first):
        one.share_from(1, p)

    own_w1.wait()

    def up(p):
        for src in range(n):
            one.ready(src, p)
        cols = at_rows(p * tile, tile)
        for share in range(2):
            @pl.loop(0, 2)
            def _(b):
                here = at_rows(b * q, q)
                total = jnp.dot(xh[0, here, :], w1s[share, 0, :, cols],
                                preferred_element_type=jnp.float32)
                for k in range(1, n):
                    total += jnp.dot(xh[k, here, :], w1s[share, k, :, cols],
                                     preferred_element_type=jnp.float32)
                h[share, here, cols] = jnp.square(jnp.maximum(total, 0.0)).astype(jnp.bfloat16)

    def far(step, ends, p):
        for o in range(2, n):
            for src in (me - o, me + o):
                end = (src == 0) | (src == n - 1)

                @pl.when((src >= 0) & (src < n) & (end if ends else jnp.logical_not(end)))
                def _():
                    step(src, p)

    def close(step, ends, p):
        for src in (me - 1, me + 1):
            end = (src == 0) | (src == n - 1)

            @pl.when((src >= 0) & (src < n) & (end if ends else jnp.logical_not(end)))
            def _():
                step(src, p)

    groups = [(close, True, p) for p in range(first, rounds1)]
    groups += [(far, True, p) for p in range(rounds1)]
    groups += [(close, False, p) for p in range(first, rounds1)]
    groups += [(far, False, p) for p in range(rounds1)]
    done = 0

    def share_group(i):
        which, ends, p = groups[i]
        which(one.share, ends, p)

    for i, (which, ends, p) in enumerate(groups):
        which(one.forward, ends, p)
        if i == min(rounds1, len(groups) - 1):
            for src in range(n):
                @pl.when(src != me)
                def _():
                    xy_landed(src).wait_recv()
        if i >= lag_g:
            share_group(i - lag_g)
            after = i - lag_g - (len(groups) - rounds1)
            if after >= 0 and i + 1 < len(groups):
                up(after)
                done = after + 1
    ahead = jnp.where((me == 0) | (me == n - 1), min(lead, rounds2), min(lead_mid, rounds2))

    def send_two(r):
        @pl.when(r >= near)
        def _():
            two.send(r, 1, 1)
        two.send(r, 2, n - 1)

    @pl.loop(0, ahead)
    def _(r):
        send_two(r)
    for i in range(max(len(groups) - lag_g, 0), len(groups)):
        share_group(i)
        after = i - (len(groups) - rounds1)
        while done <= after:
            up(done)
            done += 1
    own_w2.wait()

    def where_of(t):
        at = lax.rem(t + 4 * n * n, n)
        return t // n, jnp.where(lax.rem(at, 2) == 0, at // 2, n - 1 - at // 2)

    def out_tile(ref, block, r):
        return ref.at[at_rows(block * q, q), at_rows(r * tile2, tile2)]

    def down(d, r):
        cols = at_rows(r * tile2, tile2)
        return (jnp.dot(h[0], w2s[0, d, :, cols], preferred_element_type=jnp.float32)
                + jnp.dot(h[1], w2s[1, d, :, cols], preferred_element_type=jnp.float32))

    def y_copy(t):
        r, d = where_of(t)
        return remote(out_tile(psend, d, r), out_tile(yrecv, d, r), y_sem.at[0, t], y_sem.at[1, t],
                      {"cb": py})

    def z_copy(t, to_right):
        r, d = where_of(t)
        to = jnp.minimum(me + 1, n - 1) if to_right else jnp.maximum(me - 1, 0)
        block = d if to_right else jnp.where(d == to, n, d)
        return remote(out_tile(zsend, d, r), out_tile(zrecv, block, r), z_sem.at[0, t],
                      z_sem.at[1 if to_right else 2, t], {"ra": to})

    def z_landed(t, to_right):
        r, d = where_of(t)
        block = d if to_right else jnp.where(d == me, n, d)
        ref = out_tile(zrecv, block, r)
        return remote(ref, ref, z_sem.at[0, t], z_sem.at[1 if to_right else 2, t], {
            "ra": jnp.maximum(me - 1, 0) if to_right else jnp.minimum(me + 1, n - 1)})

    def ag_half(owner, half, r):
        return fin.at[at_rows(slot_of(owner) * q + half * (q // 2), q // 2), at_rows(r * tile2, tile2)]

    def ag_copy(r, side):
        ref = out_tile(fin, slot_of(cb), r)
        return remote(ref, ref, ag_sem.at[0, r, side], ag_sem.at[1, r, side], {"cb": (px, py)[side]})

    def ag_landed(r, side):
        ref = out_tile(fin, slot_of((px, py)[side]), r)
        return remote(ref, ref, ag_sem.at[0, r, side], ag_sem.at[1, r, side], {"cb": (px, py)[side]})

    def ag_pass(r, side):
        ref = ag_half((py, px)[side], 1 - side, r)
        return remote(ref, ref, ag_sem.at[0, r, 2 + side], ag_sem.at[1, r, 2 + side], {
            "cb": (px, py)[side]})

    def ag_passed(r, side):
        ref = ag_half(lax.rem(px + 2, m), 1 - side, r)
        return remote(ref, ref, ag_sem.at[0, r, 2 + side], ag_sem.at[1, r, 2 + side], {
            "cb": (px, py)[side]})

    def relay_ag(r):
        for side in range(2):
            ag_landed(r, 1 - side).wait_recv()
            ag_pass(r, side).start()

    def st_copy(o, c):
        return remote(st_src, st_recv.at[me, cb], st_send.at[o, c], st_rcv.at[me, cb],
                      {"ra": lax.rem(me + o, n), "cb": lax.rem(cb + c, m)})

    def st_landed(o, c):
        z, s = lax.rem(me + o, n), lax.rem(cb + c, m)
        ref = st_recv.at[z, s]
        return remote(ref, ref, st_send.at[o, c], st_rcv.at[z, s], {"ra": z, "cb": s})

    def source_of(t):
        at = lax.rem(t, n)
        return jnp.where(at < 2, at, n + 1 - at)

    def stage_r(t):
        o = source_of(t)

        @pl.when(o > 0)
        def _():
            two.forward_from(o, t // n)

    def stage_x(t):
        o = source_of(t)

        @pl.when(o > 0)
        def _():
            two.share_from(o, t // n)

        @pl.when(o == 0)
        def _():
            two.share(me, t // n)

    def stage_a(t):
        r, d = where_of(t)
        two.ready(d, r)
        both[...] = down(d, r)
        out_tile(psend, d, r)[...] = both[at_rows((1 - yb) * q, q), :].astype(jnp.bfloat16)
        y_copy(t).start()
        out_tile(zsend, d, r)[...] = both[at_rows(yb * q, q), :].astype(jnp.bfloat16)

    def stage_z(t):
        r, d = where_of(t)
        y_copy(t).wait_recv()
        acc[...] = out_tile(zsend, d, r)[...].astype(jnp.float32) + out_tile(yrecv, d, r)[
            ...].astype(jnp.float32)

        @pl.when((me >= 1) & (d >= me))
        def _():
            z_landed(t, True).wait_recv()
            acc[...] += out_tile(zrecv, d, r)[...].astype(jnp.float32)

        @pl.when((me + 1 < n) & (d <= me))
        def _():
            z_landed(t, False).wait_recv()
            acc[...] += out_tile(zrecv, jnp.where(d == me, n, d), r)[...].astype(jnp.float32)

        @pl.when(d != me)
        def _():
            out_tile(zsend, d, r)[...] = acc[...].astype(jnp.bfloat16)

        @pl.when(d > me)
        def _():
            z_copy(t, True).start()

        @pl.when(d < me)
        def _():
            z_copy(t, False).start()

        @pl.when(d == me)
        def _():
            out_tile(fin, slot_of(cb), r)[...] = acc[...].astype(jnp.bfloat16)
            for c in range(qchunks):
                sums = sums_of(acc[pl.ds(c * 128, 128), :] + residual_scale * xres[
                    at_rows(slot_of(cb) * q + c * 128, 128), at_rows(r * tile2, tile2)].astype(
                        jnp.float32))
                st_src[pl.ds(c, 1), :] += sums[0:1, :]
                st_src[pl.ds(qchunks + c, 1), :] += sums[64:65, :]

            @pl.when(r == rounds2 - 1)
            def _():
                for o in range(n):
                    for c in range(m):
                        if o or c:
                            st_copy(o, c).start()
            for side in range(2):
                ag_copy(r, side).start()

            @pl.when(r > 0)
            def _():
                relay_ag(r - 1)

    def lag_of(hop):
        return lag_z + hop * lag_hop + jnp.where(2 * hop >= n, lag_late, 0)

    @pl.loop(0, tiles + lag_z + (n - 1) * lag_hop + lag_late)
    def _(step):
        for lag, stage in ((0, stage_r), (lag_x, stage_x), (lag_a, stage_a)):
            @pl.when((step >= lag) & (step < tiles + lag))
            def _():
                stage(step - lag)
            if stage is stage_r:
                late = (step + 1) // n - 1 + ahead

                @pl.when((lax.rem(step + 1, n) == 0) & (late < rounds2))
                def _():
                    send_two(late)

        @pl.loop(0, n)
        def _(back):
            hop = n - 1 - back
            t = step - lag_of(hop)
            d = where_of(t)[1]
            mine = jnp.where(d > me, me, jnp.where(
                d < me, n - 1 - me, jnp.maximum(me, n - 1 - me)))

            @pl.when((t >= 0) & (t < tiles) & (mine == hop))
            def _():
                stage_z(t)

    relay_ag(rounds2 - 1)
    for src in range(n):
        @pl.when((src == me) | (src < me))
        def _():
            @pl.when(me + 1 < n)
            def _():
                xz(src, True).wait_send()

        @pl.when((src == me) | (src > me))
        def _():
            @pl.when(me >= 1)
            def _():
                xz(src, False).wait_send()

        @pl.when(src != me)
        def _():
            xy(src).wait_send()

        for stream, count in ((one, rounds1), (two, rounds2)):
            @pl.loop(0, count)
            def _(p):
                stream.sent(src, p)
    for o in range(1, n):
        s1_copy(o).wait_send()

    @pl.loop(0, tiles)
    def _(t):
        d = where_of(t)[1]
        y_copy(t).wait_send()

        @pl.when(d != me)
        def _():
            z_copy(t, True).wait_send()

    for o in range(n):
        for c in range(m):
            if o or c:
                st_landed(o, c).wait_recv()
    st_recv[me, cb] = st_src[...]
    for side in range(2):
        @pl.loop(0, rounds2)
        def _(r):
            ag_passed(r, side).wait_recv()

    def out_copy(c):
        here = at_rows(c * 128, 128)
        return pltpu.make_async_copy(xres.at[here], o_hbm.at[here], out_sem.at[c])

    for slot in range(m):
        owner = slot // 2 + 2 * (slot % 2)
        total = st_recv[0, owner]
        for z in range(1, n):
            total += st_recv[z, owner]
        s1_tot[pl.ds(0, 2 * qchunks), :] = total[0:2 * qchunks, :]

        @pl.loop(0, qchunks)
        def _(c):
            mean_row = s1_tot[pl.ds(c, 1), :] / width
            scale_row = lax.rsqrt(
                s1_tot[pl.ds(qchunks + c, 1), :] / width - mean_row * mean_row + norm_eps)
            mean, scale = column(mean_row), column(scale_row)
            for part in range(4):
                here = at_rows(slot * q + c * 128 + part * 32, 32)
                own = slice(part * 32, part * 32 + 32)
                mixed = residual_scale * xres[here, :].astype(jnp.float32) + fin[here, :].astype(
                    jnp.float32)
                xres[here, :] = ((mixed - mean[own]) * scale[own] * gain_ref[...]
                                 + bias_ref[...]).astype(jnp.bfloat16)
            out_copy(slot * qchunks + c).start()

    for side in range(2):
        @pl.loop(0, rounds2)
        def _(r):
            ag_copy(r, side).wait_send()
            ag_pass(r, side).wait_send()
    for o in range(n):
        for c in range(m):
            if o or c:
                st_copy(o, c).wait_send()

    @pl.loop(0, chunks)
    def _(c):
        out_copy(c).wait()


def per_device(carried, branch_in, gain_in, bias_in, up_weight, down_weight, gain_out, bias_out):
    n, m, nd = lax.axis_size("ra"), lax.axis_size("cb"), lax.axis_size("dp")
    tokens, dl = carried.shape
    fs = up_weight.shape[1] // n
    assert m == 4 and nd == 2 and tokens % (128 * m) == 0 and tokens // m <= 512
    q = tokens // m
    tile = math.gcd(tile_cap, math.gcd(fs, dl))
    tile2 = math.gcd(tile2_cap, dl)
    rounds1, rounds2 = fs // tile, dl // tile2
    tiles = rounds2 * n
    chunk_rows = -(-2 * (tokens // 128) // 8) * 8
    dma = pltpu.SemaphoreType.DMA
    bf16, f32 = jnp.bfloat16, jnp.float32
    hbm = pl.BlockSpec(memory_space=pl.ANY)
    vmem = pl.BlockSpec(memory_space=pltpu.VMEM)
    return pl.pallas_call(
        functools.partial(kernel, n, m, tile, tile2),
        out_shape=jax.ShapeDtypeStruct((tokens, dl), bf16),
        in_specs=[hbm, hbm, hbm, hbm, vmem, vmem, vmem, vmem],
        out_specs=hbm,
        scratch_shapes=[
            pltpu.VMEM((chunk_rows, 128), f32),
            pltpu.VMEM((n, chunk_rows, 128), f32),
            pltpu.VMEM((chunk_rows, 128), f32),
            pltpu.VMEM((n, 2 * q, dl), bf16),
            pltpu.VMEM((tokens, dl), bf16),
            pltpu.VMEM((2, n, dl, fs), bf16),
            pltpu.VMEM((2, n, fs, dl), bf16),
            pltpu.VMEM((2, 2 * q, fs), bf16),
            pltpu.VMEM((max(n, m) * q, dl), bf16),
            pltpu.VMEM((n * q, dl), bf16),
            pltpu.VMEM((n * q, dl), bf16),
            pltpu.VMEM(((n + 1) * q, dl), bf16),
            pltpu.VMEM((tokens, dl), bf16),
            pltpu.VMEM((2 * q, tile2), f32),
            pltpu.VMEM((q, tile2), f32),
            pltpu.VMEM((8, 128), f32),
            pltpu.VMEM((n, m, 8, 128), f32),
            dma((4,)), dma((2, n)), dma((8, n, rounds1)), dma((8, n, rounds2)), dma((3, n)),
            dma((2, n)), dma((2, tiles)), dma((3, tiles)), dma((2, rounds2, m)), dma((n, m)),
            dma((n, m)), dma((tokens // 128,)), pltpu.SemaphoreType.REGULAR,
        ],
        compiler_params=pltpu.CompilerParams(
            collective_id=0, has_side_effects=True, vmem_limit_bytes=67 * 1000 * 1000),
    )(carried, branch_in, up_weight, down_weight, gain_in.reshape(1, dl), bias_in.reshape(1, dl),
      gain_out.reshape(1, dl), bias_out.reshape(1, dl))


def solution(mesh):
    in_specs = (
        P("dp", "ra"),
        P("dp", "ra"),
        P("ra"),
        P("ra"),
        P("ra", "cb"),
        P("cb", "ra"),
        P("ra"),
        P("ra"),
    )
    out_specs = P("dp", "ra")
    return jax.shard_map(
        per_device, mesh=mesh, in_specs=in_specs, out_specs=out_specs, check_vma=False
    )
```

```python
import functools
import math

import jax
import jax.numpy as jnp
from jax import lax
from jax.experimental import pallas as pl
from jax.experimental.pallas import tpu as pltpu
from jax.sharding import PartitionSpec as P

residual_scale = 2.0**0.25
norm_eps = 1e-05
tile_cap = 256
tile2_cap = 128
lag_x, lag_a, lag_z, lag_hop, lag_late = 3, 7, 14, 8, 0
lead = 3
lead_mid = 5
near = 3
early = 2
lag_g = 1


def kernel(n, m, tile, tile2, carried_hbm, branch_hbm, w1_hbm, w2_hbm, gain_in_ref, bias_in_ref, gain_ref,
           bias_ref, o_hbm, s1_src, s1_recv, s1_tot, xh, xres, w1s, w2s, h, psend, yrecv, zsend,
           zrecv, fin, both, acc, st_src, st_recv, loc_sem, s1_sem, w1_sem, w2_sem, xz_sem, xy_sem,
           y_sem, z_sem, ag_sem, st_send, st_rcv, out_sem, meet_sem):
    me, cb, dp = lax.axis_index("ra"), lax.axis_index("cb"), lax.axis_index("dp")
    tokens, dl = xres.shape
    fs = h.shape[2]
    q = tokens // m
    chunks = tokens // 128
    qchunks = q // 128
    rounds1, rounds2 = fs // tile, dl // tile2
    tiles = rounds2 * n
    first = min(early, rounds1)
    width = n * dl
    xb, yb = lax.rem(cb, 2), cb // 2
    px, py = cb + 1 - 2 * xb, lax.rem(cb + 2, m)
    sib = 1 - dp

    def slot_of(c):
        return lax.rem(c, 2) * 2 + c // 2

    def at_rows(start, size):
        return pl.ds(pl.multiple_of(start, size), size)

    def remote(src, dst, send, recv, to):
        return pltpu.make_async_remote_copy(
            src_ref=src, dst_ref=dst, send_sem=send, recv_sem=recv, device_id=to)

    barrier = pltpu.get_barrier_semaphore()
    for o in range(n):
        for c in range(m):
            if o or c:
                pl.semaphore_signal(barrier, inc=1, device_id={
                    "ra": lax.rem(me + o, n), "cb": lax.rem(cb + c, m)})
    pl.semaphore_signal(barrier, inc=1, device_id={"dp": sib})

    own_carried = pltpu.make_async_copy(carried_hbm, fin, loc_sem.at[0])
    own_branch = pltpu.make_async_copy(branch_hbm, psend.at[pl.ds(0, tokens)], loc_sem.at[1])
    own_w1 = pltpu.make_async_copy(w1_hbm.at[:, at_rows(me * fs, fs)], w1s.at[0, me], loc_sem.at[2])
    own_w2 = pltpu.make_async_copy(w2_hbm.at[at_rows(me * fs, fs)], w2s.at[0, me], loc_sem.at[3])
    own_carried.start()
    own_branch.start()
    own_w1.start()
    own_w2.start()
    pl.semaphore_wait(barrier, n * m)

    class Stream:
        def __init__(self, buf, sem, tile, block):
            self.buf, self.sem, self.tile, self.block = buf, sem, tile, block
            half = buf.shape[2] // 2
            self.rows = at_rows(dp * half, half)
            self.other = at_rows(sib * half, half)

        def ref(self, share, src, p, rows):
            return self.buf.at[share, src, rows, at_rows(p * self.tile, self.tile)]

        def z(self, to, p):
            return remote(self.block(to, p), self.ref(0, me, p, self.rows),
                          self.sem.at[0, to, p], self.sem.at[1, me, p], {"ra": to})

        def z_landed(self, src, p):
            ref = self.ref(0, src, p, self.rows)
            return remote(ref, ref, self.sem.at[0, src, p], self.sem.at[1, src, p], {"ra": src})

        def x(self, src, p):
            ref = self.ref(0, src, p, self.rows)
            return remote(ref, self.ref(1, src, p, self.rows), self.sem.at[2, src, p],
                          self.sem.at[3, src, p], {"cb": px})

        def x_own(self, p):
            return remote(self.block(me, p), self.ref(1, me, p, self.rows), self.sem.at[2, me, p],
                          self.sem.at[3, me, p], {"cb": px})

        def pair(self, share, src, p):
            ref = self.ref(share, src, p, self.rows)
            return remote(ref, ref, self.sem.at[4 + 2 * share, src, p],
                          self.sem.at[5 + 2 * share, src, p], {"dp": sib})

        def pair_landed(self, share, src, p):
            ref = self.ref(share, src, p, self.other)
            return remote(ref, ref, self.sem.at[4 + 2 * share, src, p],
                          self.sem.at[5 + 2 * share, src, p], {"dp": sib})

        def right(self, p, least, most):
            for o in range(least, most + 1):
                @pl.when(me + o < n)
                def _():
                    self.z(me + o, p).start()

        def left(self, p, least, most):
            for o in range(least, most + 1):
                @pl.when(me >= o)
                def _():
                    self.z(me - o, p).start()

        def send(self, p, least=1, most=n - 1):
            for o in range(least, most + 1):
                self.right(p, o, o)
                self.left(p, o, o)

        def forward(self, src, p):
            self.z_landed(src, p).wait_recv()
            self.x(src, p).start()
            self.pair(0, src, p).start()

        def forward_from(self, o, p):
            @pl.when(me + o < n)
            def _():
                self.forward(me + o, p)

            @pl.when(me >= o)
            def _():
                self.forward(me - o, p)

        def share_from(self, o, p):
            @pl.when(me + o < n)
            def _():
                self.share(me + o, p)

            @pl.when(me >= o)
            def _():
                self.share(me - o, p)

        def share(self, src, p):
            self.x(src, p).wait_recv()
            self.pair(1, src, p).start()

        def ready(self, src, p):
            @pl.when(src != me)
            def _():
                self.pair_landed(0, src, p).wait_recv()
            self.pair_landed(1, src, p).wait_recv()

        def sent(self, src, p):
            @pl.when(src != me)
            def _():
                self.z(src, p).wait_send()
                self.pair(0, src, p).wait_send()
            self.x(src, p).wait_send()
            self.pair(1, src, p).wait_send()

    one = Stream(w1s, w1_sem, tile, lambda to, p: w1_hbm.at[
        at_rows(dp * (dl // 2), dl // 2), at_rows(to * fs + p * tile, tile)])
    two = Stream(w2s, w2_sem, tile2, lambda to, p: w2_hbm.at[
        at_rows(to * fs + dp * (fs // 2), fs // 2), at_rows(p * tile2, tile2)])

    one.send(0, 1, 1)
    for p in range(rounds1):
        one.x_own(p).start()

    def s1_copy(o):
        return remote(s1_src, s1_recv.at[me], s1_sem.at[0, o], s1_sem.at[1, me],
                      {"ra": lax.rem(me + o, n)})

    def s1_landed(o):
        sender = lax.rem(me + o, n)
        ref = s1_recv.at[sender]
        return remote(ref, ref, s1_sem.at[0, o], s1_sem.at[1, sender], {"ra": sender})

    def mixed_in(here):
        return residual_scale * fin[here, :].astype(jnp.float32) + psend[here, :].astype(
            jnp.float32)

    def sums_of(total):
        lane = lax.broadcasted_iota(jnp.int32, (128, 128), 1)
        return jnp.where(
            lane < 64, jnp.sum(total, axis=1, keepdims=True),
            jnp.sum(total * total, axis=1, keepdims=True)).T

    def column(row):
        return jnp.broadcast_to(row, (128, 128)).T[:, 0:1]

    st_src[...] = jnp.zeros_like(st_src)
    own_carried.wait()
    own_branch.wait()

    @pl.loop(0, chunks)
    def _(c):
        sums = sums_of(mixed_in(at_rows(c * 128, 128)))
        s1_src[pl.ds(c, 1), :] = sums[0:1, :]
        s1_src[pl.ds(chunks + c, 1), :] = sums[64:65, :]
    for o in range(1, n):
        s1_copy(o).start()
    for p in range(1, first):
        one.send(p, 1, 1)
    s1_tot[...] = s1_src[...]
    for o in range(1, n):
        s1_landed(o).wait_recv()
        s1_tot[...] += s1_recv[lax.rem(me + o, n)]

    def normed(c, local=None):
        mean_row = s1_tot[pl.ds(c, 1), :] / width
        scale_row = lax.rsqrt(s1_tot[pl.ds(chunks + c, 1), :] / width - mean_row * mean_row + norm_eps)
        mean, scale = column(mean_row), column(scale_row)
        for part in range(4):
            here = at_rows(c * 128 + part * 32, 32)
            own = slice(part * 32, part * 32 + 32)
            out = ((mixed_in(here) - mean[own]) * scale[own] * gain_in_ref[...]
                   + bias_in_ref[...]).astype(jnp.bfloat16)
            xres[here, :] = out
            if local is not None:
                xh[me, at_rows(local * 128 + part * 32, 32), :] = out

    def normed_half(first, count):
        @pl.loop(0, count)
        def _(c):
            local = first + c
            normed(xb * 2 * qchunks + local, local)

    normed_half(yb * qchunks, qchunks)

    def xz(src, to_right):
        ref = xh.at[src, at_rows(yb * q, q)]
        return remote(ref, ref, xz_sem.at[0 if to_right else 1, src], xz_sem.at[2, src], {
            "ra": jnp.minimum(me + 1, n - 1) if to_right else jnp.maximum(me - 1, 0)})

    def xy(src):
        ref = xh.at[src, at_rows(yb * q, q)]
        return remote(ref, ref, xy_sem.at[0, src], xy_sem.at[1, src], {"cb": py})

    def xy_landed(src):
        ref = xh.at[src, at_rows((1 - yb) * q, q)]
        return remote(ref, ref, xy_sem.at[0, src], xy_sem.at[1, src], {"cb": py})

    def from_left(s):
        @pl.when(me >= s)
        def _():
            xz(me - s, True).wait_recv()

            @pl.when(me + 1 < n)
            def _():
                xz(me - s, True).start()
            xy(me - s).start()

    def from_right(s):
        @pl.when(me + s < n)
        def _():
            xz(me + s, False).wait_recv()

            @pl.when(me >= 1)
            def _():
                xz(me + s, False).start()
            xy(me + s).start()

    def meet():
        pl.semaphore_signal(meet_sem, inc=1, device_id={"dp": sib})
        pl.semaphore_wait(meet_sem, 1)

    def after_relays(s):
        @pl.when(me == s)
        def _():
            for p in range(first, rounds1):
                one.right(p, 1, 1)

        @pl.when(me == n - 1 - s)
        def _():
            for p in range(first, rounds1):
                one.left(p, 1, 1)
        for o in range(2, n):
            @pl.when(me + o == s)
            def _():
                for p in range(rounds1):
                    one.right(p, o, o)

            @pl.when(me - o == n - 1 - s)
            def _():
                for p in range(rounds1):
                    one.left(p, o, o)

    @pl.when(me + 1 < n)
    def _():
        xz(me, True).start()

    @pl.when(me >= 1)
    def _():
        xz(me, False).start()
    after_relays(0)
    normed_half((1 - yb) * qchunks, qchunks)

    @pl.loop(0, 2 * qchunks)
    def _(c):
        normed((1 - xb) * 2 * qchunks + c)

    for p in range(first):
        one.forward_from(1, p)
    for p in range(rounds2):
        two.x_own(p).start()
    for s in range(1, n):
        from_left(s)
        from_right(s)
        meet()
        after_relays(s)
    for p in range(min(near, rounds2)):
        two.send(p, 1, 1)
    for p in range(rounds1):
        one.share(me, p)
    for p in range(first):
        one.share_from(1, p)

    own_w1.wait()

    def up(p):
        for src in range(n):
            one.ready(src, p)
        cols = at_rows(p * tile, tile)
        for share in range(2):
            @pl.loop(0, 2)
            def _(b):
                here = at_rows(b * q, q)
                total = jnp.dot(xh[0, here, :], w1s[share, 0, :, cols],
                                preferred_element_type=jnp.float32)
                for k in range(1, n):
                    total += jnp.dot(xh[k, here, :], w1s[share, k, :, cols],
                                     preferred_element_type=jnp.float32)
                h[share, here, cols] = jnp.square(jnp.maximum(total, 0.0)).astype(jnp.bfloat16)

    def far(step, ends, p):
        for o in range(2, n):
            for src in (me - o, me + o):
                end = (src == 0) | (src == n - 1)

                @pl.when((src >= 0) & (src < n) & (end if ends else jnp.logical_not(end)))
                def _():
                    step(src, p)

    def close(step, ends, p):
        for src in (me - 1, me + 1):
            end = (src == 0) | (src == n - 1)

            @pl.when((src >= 0) & (src < n) & (end if ends else jnp.logical_not(end)))
            def _():
                step(src, p)

    groups = [(close, True, p) for p in range(first, rounds1)]
    groups += [(far, True, p) for p in range(rounds1)]
    groups += [(close, False, p) for p in range(first, rounds1)]
    groups += [(far, False, p) for p in range(rounds1)]
    done = 0

    def share_group(i):
        which, ends, p = groups[i]
        which(one.share, ends, p)

    for i, (which, ends, p) in enumerate(groups):
        which(one.forward, ends, p)
        if i == min(rounds1, len(groups) - 1):
            for src in range(n):
                @pl.when(src != me)
                def _():
                    xy_landed(src).wait_recv()
        if i >= lag_g:
            share_group(i - lag_g)
            after = i - lag_g - (len(groups) - rounds1)
            if after >= 0 and i + 1 < len(groups):
                up(after)
                done = after + 1
    ahead = jnp.where((me == 0) | (me == n - 1), min(lead, rounds2), min(lead_mid, rounds2))

    def send_two(r):
        @pl.when(r >= near)
        def _():
            two.send(r, 1, 1)
        two.send(r, 2, n - 1)

    @pl.loop(0, ahead)
    def _(r):
        send_two(r)
    for i in range(max(len(groups) - lag_g, 0), len(groups)):
        share_group(i)
        after = i - (len(groups) - rounds1)
        while done <= after:
            up(done)
            done += 1
    own_w2.wait()

    def where_of(t):
        at = lax.rem(t + 4 * n * n, n)
        return t // n, jnp.where(lax.rem(at, 2) == 0, at // 2, n - 1 - at // 2)

    def out_tile(ref, block, r):
        return ref.at[at_rows(block * q, q), at_rows(r * tile2, tile2)]

    def down(d, r):
        cols = at_rows(r * tile2, tile2)
        return (jnp.dot(h[0], w2s[0, d, :, cols], preferred_element_type=jnp.float32)
                + jnp.dot(h[1], w2s[1, d, :, cols], preferred_element_type=jnp.float32))

    def y_copy(t):
        r, d = where_of(t)
        return remote(out_tile(psend, d, r), out_tile(yrecv, d, r), y_sem.at[0, t], y_sem.at[1, t],
                      {"cb": py})

    def z_copy(t, to_right):
        r, d = where_of(t)
        to = jnp.minimum(me + 1, n - 1) if to_right else jnp.maximum(me - 1, 0)
        block = d if to_right else jnp.where(d == to, n, d)
        return remote(out_tile(zsend, d, r), out_tile(zrecv, block, r), z_sem.at[0, t],
                      z_sem.at[1 if to_right else 2, t], {"ra": to})

    def z_landed(t, to_right):
        r, d = where_of(t)
        block = d if to_right else jnp.where(d == me, n, d)
        ref = out_tile(zrecv, block, r)
        return remote(ref, ref, z_sem.at[0, t], z_sem.at[1 if to_right else 2, t], {
            "ra": jnp.maximum(me - 1, 0) if to_right else jnp.minimum(me + 1, n - 1)})

    def ag_half(owner, half, r):
        return fin.at[at_rows(slot_of(owner) * q + half * (q // 2), q // 2), at_rows(r * tile2, tile2)]

    def ag_copy(r, side):
        ref = out_tile(fin, slot_of(cb), r)
        return remote(ref, ref, ag_sem.at[0, r, side], ag_sem.at[1, r, side], {"cb": (px, py)[side]})

    def ag_landed(r, side):
        ref = out_tile(fin, slot_of((px, py)[side]), r)
        return remote(ref, ref, ag_sem.at[0, r, side], ag_sem.at[1, r, side], {"cb": (px, py)[side]})

    def ag_pass(r, side):
        ref = ag_half((py, px)[side], 1 - side, r)
        return remote(ref, ref, ag_sem.at[0, r, 2 + side], ag_sem.at[1, r, 2 + side], {
            "cb": (px, py)[side]})

    def ag_passed(r, side):
        ref = ag_half(lax.rem(px + 2, m), 1 - side, r)
        return remote(ref, ref, ag_sem.at[0, r, 2 + side], ag_sem.at[1, r, 2 + side], {
            "cb": (px, py)[side]})

    def relay_ag(r):
        for side in range(2):
            ag_landed(r, 1 - side).wait_recv()
            ag_pass(r, side).start()

    def st_copy(o, c):
        return remote(st_src, st_recv.at[me, cb], st_send.at[o, c], st_rcv.at[me, cb],
                      {"ra": lax.rem(me + o, n), "cb": lax.rem(cb + c, m)})

    def st_landed(o, c):
        z, s = lax.rem(me + o, n), lax.rem(cb + c, m)
        ref = st_recv.at[z, s]
        return remote(ref, ref, st_send.at[o, c], st_rcv.at[z, s], {"ra": z, "cb": s})

    def source_of(t):
        at = lax.rem(t, n)
        return jnp.where(at < 2, at, n + 1 - at)

    def stage_r(t):
        o = source_of(t)

        @pl.when(o > 0)
        def _():
            two.forward_from(o, t // n)

    def stage_x(t):
        o = source_of(t)

        @pl.when(o > 0)
        def _():
            two.share_from(o, t // n)

        @pl.when(o == 0)
        def _():
            two.share(me, t // n)

    def stage_a(t):
        r, d = where_of(t)
        two.ready(d, r)
        both[...] = down(d, r)
        out_tile(psend, d, r)[...] = both[at_rows((1 - yb) * q, q), :].astype(jnp.bfloat16)
        y_copy(t).start()
        out_tile(zsend, d, r)[...] = both[at_rows(yb * q, q), :].astype(jnp.bfloat16)

    def stage_z(t):
        r, d = where_of(t)
        y_copy(t).wait_recv()
        acc[...] = out_tile(zsend, d, r)[...].astype(jnp.float32) + out_tile(yrecv, d, r)[
            ...].astype(jnp.float32)

        @pl.when((me >= 1) & (d >= me))
        def _():
            z_landed(t, True).wait_recv()
            acc[...] += out_tile(zrecv, d, r)[...].astype(jnp.float32)

        @pl.when((me + 1 < n) & (d <= me))
        def _():
            z_landed(t, False).wait_recv()
            acc[...] += out_tile(zrecv, jnp.where(d == me, n, d), r)[...].astype(jnp.float32)

        @pl.when(d != me)
        def _():
            out_tile(zsend, d, r)[...] = acc[...].astype(jnp.bfloat16)

        @pl.when(d > me)
        def _():
            z_copy(t, True).start()

        @pl.when(d < me)
        def _():
            z_copy(t, False).start()

        @pl.when(d == me)
        def _():
            out_tile(fin, slot_of(cb), r)[...] = acc[...].astype(jnp.bfloat16)
            for c in range(qchunks):
                sums = sums_of(acc[pl.ds(c * 128, 128), :] + residual_scale * xres[
                    at_rows(slot_of(cb) * q + c * 128, 128), at_rows(r * tile2, tile2)].astype(
                        jnp.float32))
                st_src[pl.ds(c, 1), :] += sums[0:1, :]
                st_src[pl.ds(qchunks + c, 1), :] += sums[64:65, :]

            @pl.when(r == rounds2 - 1)
            def _():
                for o in range(n):
                    for c in range(m):
                        if o or c:
                            st_copy(o, c).start()
            for side in range(2):
                ag_copy(r, side).start()

            @pl.when(r > 0)
            def _():
                relay_ag(r - 1)

    def lag_of(hop):
        return lag_z + hop * lag_hop + jnp.where(2 * hop >= n, lag_late, 0)

    @pl.loop(0, tiles + lag_z + (n - 1) * lag_hop + lag_late)
    def _(step):
        for lag, stage in ((0, stage_r), (lag_x, stage_x), (lag_a, stage_a)):
            @pl.when((step >= lag) & (step < tiles + lag))
            def _():
                stage(step - lag)
            if stage is stage_r:
                late = (step + 1) // n - 1 + ahead

                @pl.when((lax.rem(step + 1, n) == 0) & (late < rounds2))
                def _():
                    send_two(late)

        @pl.loop(0, n)
        def _(back):
            hop = n - 1 - back
            t = step - lag_of(hop)
            d = where_of(t)[1]
            mine = jnp.where(d > me, me, jnp.where(
                d < me, n - 1 - me, jnp.maximum(me, n - 1 - me)))

            @pl.when((t >= 0) & (t < tiles) & (mine == hop))
            def _():
                stage_z(t)

    relay_ag(rounds2 - 1)
    for src in range(n):
        @pl.when((src == me) | (src < me))
        def _():
            @pl.when(me + 1 < n)
            def _():
                xz(src, True).wait_send()

        @pl.when((src == me) | (src > me))
        def _():
            @pl.when(me >= 1)
            def _():
                xz(src, False).wait_send()

        @pl.when(src != me)
        def _():
            xy(src).wait_send()

        for stream, count in ((one, rounds1), (two, rounds2)):
            @pl.loop(0, count)
            def _(p):
                stream.sent(src, p)
    for o in range(1, n):
        s1_copy(o).wait_send()

    @pl.loop(0, tiles)
    def _(t):
        d = where_of(t)[1]
        y_copy(t).wait_send()

        @pl.when(d != me)
        def _():
            z_copy(t, True).wait_send()

    for o in range(n):
        for c in range(m):
            if o or c:
                st_landed(o, c).wait_recv()
    st_recv[me, cb] = st_src[...]
    for side in range(2):
        @pl.loop(0, rounds2)
        def _(r):
            ag_passed(r, side).wait_recv()

    def out_copy(c):
        here = at_rows(c * 128, 128)
        return pltpu.make_async_copy(xres.at[here], o_hbm.at[here], out_sem.at[c])

    for slot in range(m):
        owner = slot // 2 + 2 * (slot % 2)
        total = st_recv[0, owner]
        for z in range(1, n):
            total += st_recv[z, owner]
        s1_tot[pl.ds(0, 2 * qchunks), :] = total[0:2 * qchunks, :]

        @pl.loop(0, qchunks)
        def _(c):
            mean_row = s1_tot[pl.ds(c, 1), :] / width
            scale_row = lax.rsqrt(
                s1_tot[pl.ds(qchunks + c, 1), :] / width - mean_row * mean_row + norm_eps)
            mean, scale = column(mean_row), column(scale_row)
            for part in range(4):
                here = at_rows(slot * q + c * 128 + part * 32, 32)
                own = slice(part * 32, part * 32 + 32)
                mixed = residual_scale * xres[here, :].astype(jnp.float32) + fin[here, :].astype(
                    jnp.float32)
                xres[here, :] = ((mixed - mean[own]) * scale[own] * gain_ref[...]
                                 + bias_ref[...]).astype(jnp.bfloat16)
            out_copy(slot * qchunks + c).start()

    for side in range(2):
        @pl.loop(0, rounds2)
        def _(r):
            ag_copy(r, side).wait_send()
            ag_pass(r, side).wait_send()
    for o in range(n):
        for c in range(m):
            if o or c:
                st_copy(o, c).wait_send()

    @pl.loop(0, chunks)
    def _(c):
        out_copy(c).wait()


def per_device(carried, branch_in, gain_in, bias_in, up_weight, down_weight, gain_out, bias_out):
    n, m, nd = lax.axis_size("ra"), lax.axis_size("cb"), lax.axis_size("dp")
    tokens, dl = carried.shape
    fs = up_weight.shape[1] // n
    assert m == 4 and nd == 2 and tokens % (128 * m) == 0 and tokens // m <= 512
    q = tokens // m
    tile = math.gcd(tile_cap, math.gcd(fs, dl))
    tile2 = math.gcd(tile2_cap, dl)
    rounds1, rounds2 = fs // tile, dl // tile2
    tiles = rounds2 * n
    chunk_rows = -(-2 * (tokens // 128) // 8) * 8
    dma = pltpu.SemaphoreType.DMA
    bf16, f32 = jnp.bfloat16, jnp.float32
    hbm = pl.BlockSpec(memory_space=pl.ANY)
    vmem = pl.BlockSpec(memory_space=pltpu.VMEM)
    return pl.pallas_call(
        functools.partial(kernel, n, m, tile, tile2),
        out_shape=jax.ShapeDtypeStruct((tokens, dl), bf16),
        in_specs=[hbm, hbm, hbm, hbm, vmem, vmem, vmem, vmem],
        out_specs=hbm,
        scratch_shapes=[
            pltpu.VMEM((chunk_rows, 128), f32),
            pltpu.VMEM((n, chunk_rows, 128), f32),
            pltpu.VMEM((chunk_rows, 128), f32),
            pltpu.VMEM((n, 2 * q, dl), bf16),
            pltpu.VMEM((tokens, dl), bf16),
            pltpu.VMEM((2, n, dl, fs), bf16),
            pltpu.VMEM((2, n, fs, dl), bf16),
            pltpu.VMEM((2, 2 * q, fs), bf16),
            pltpu.VMEM((max(n, m) * q, dl), bf16),
            pltpu.VMEM((n * q, dl), bf16),
            pltpu.VMEM((n * q, dl), bf16),
            pltpu.VMEM(((n + 1) * q, dl), bf16),
            pltpu.VMEM((tokens, dl), bf16),
            pltpu.VMEM((2 * q, tile2), f32),
            pltpu.VMEM((q, tile2), f32),
            pltpu.VMEM((8, 128), f32),
            pltpu.VMEM((n, m, 8, 128), f32),
            dma((4,)), dma((2, n)), dma((8, n, rounds1)), dma((8, n, rounds2)), dma((3, n)),
            dma((2, n)), dma((2, tiles)), dma((3, tiles)), dma((2, rounds2, m)), dma((n, m)),
            dma((n, m)), dma((tokens // 128,)), pltpu.SemaphoreType.REGULAR,
        ],
        compiler_params=pltpu.CompilerParams(
            collective_id=0, has_side_effects=True, vmem_limit_bytes=67 * 1000 * 1000),
    )(carried, branch_in, up_weight, down_weight, gain_in.reshape(1, dl), bias_in.reshape(1, dl),
      gain_out.reshape(1, dl), bias_out.reshape(1, dl))


def solution(mesh):
    in_specs = (
        P("dp", "ra"),
        P("dp", "ra"),
        P("ra"),
        P("ra"),
        P("ra", "cb"),
        P("cb", "ra"),
        P("ra"),
        P("ra"),
    )
    out_specs = P("dp", "ra")
    return jax.shard_map(
        per_device, mesh=mesh, in_specs=in_specs, out_specs=out_specs, check_vma=False
    )
```
